32 devices in a mesh: grp: 2 (over y), sp: 4 (over z), tp: 4 (over x, core).
Axes of the slice: x: 2, y: 2, z: 4, core: 2. Of those that a mesh axis runs over, the one named last changes fastest.
Arguments:
- query_nope: bfloat16 [2560, 1024], P(('grp', 'sp'), 'tp'), parts along dimension 0, may hold values from -12 to 12
- query_rope: bfloat16 [2560, 512], P(('grp', 'sp'), 'tp'), parts along dimension 0, may hold values from -48 to 48
- token_latent: bfloat16 [2560, 256], P(('grp', 'sp')), parts along dimension 0, may hold values from -6 to 6
- key_rope: bfloat16 [2560, 32], P(('grp', 'sp')), parts along dimension 0, may hold values from -48 to 48
- latent_norm_gain: float32 [256], replicated, may hold values from 0.1 to 1.9
- key_expand_weight: bfloat16 [256, 1024], replicated, may hold values from -0.375 to 0.375
- value_expand_weight: bfloat16 [256, 1024], replicated, may hold values from -0.375 to 0.375
- residual: bfloat16 [2560, 2048], P(('grp', 'sp')), parts along dimension 0, may hold values from -3 to 3
- out_weight: bfloat16 [1024, 2048], P('tp'), may hold values from -0.375 to 0.375
- ffn_gain: float32 [2048], replicated, may hold values from 0.1 to 1.9
- gate_weight: bfloat16 [2048, 5632], P('sp', 'tp'), may hold values from -0.125 to 0.125
- up_weight: bfloat16 [2048, 5632], P('sp', 'tp'), may hold values from -0.125 to 0.125
- down_weight: bfloat16 [5632, 2048], P('tp', 'sp'), may hold values from -0.078125 to 0.078125
Outputs:
- layer_output: bfloat16 [2560, 2048], P(('grp', 'sp', 'tp')), parts along dimension 0
The draws below stay inside these ranges and needn't reach their ends.
There are 2 independent parts, one for each index of `grp`. The reference program is written for one: setup_inputs(seed, part) draws one part's arguments, and reference() takes and returns one part's arrays. A program takes and returns all parts, laid end to end along the dimension named above; an argument that names none is the same for every part. Nothing has to cross between parts.
All inputs are finite; a program needn't handle non-finite values.
Results may differ from the reference program's by a relative error of at most 0.015.
Values may be sent and summed in bfloat16 or wider, within the bound.
A program may use at most 128 MiB of HBM per device.

```python
import math
import jax
import jax.numpy as jnp
from jax import lax

D = 2048
HEAD_COUNT = 16
UNROTATED_SIZE = 64
ROPE = 32
VALUE_SIZE = 64
LATENT_RANK = 256
FF = 5632
GRID_W = 64
TOKEN_COUNT = 1280
N_TP = 4


def rope_pair(key):
    base = jax.random.fold_in(key, 29)
    streams = jax.random.split(base, 2)
    key_rope = jax.random.normal(streams[0], (TOKEN_COUNT, ROPE), jnp.float32)
    query_rope = 2.5 * jax.random.normal(streams[1], (TOKEN_COUNT, HEAD_COUNT * ROPE), jnp.float32)
    return (jnp.clip(key_rope, -48.0, 48.0), jnp.clip(query_rope, -48.0, 48.0))


def draw_query_rope(key, part):
    return rope_pair(key)[1].astype(jnp.bfloat16)


def draw_key_rope(key, part):
    return rope_pair(key)[0].astype(jnp.bfloat16)


def level_of(stream_key, shape, shards, low, high):
    level, own = 1.0, jax.random.fold_in(stream_key, 6)
    for axis_at, shards_of in shards:
        heights = jnp.exp(jax.random.uniform(jax.random.fold_in(own, axis_at), (shards_of,), jnp.float32, low / len(shards), high / len(shards)))
        level = level * jnp.repeat(heights, shape[axis_at] // shards_of).reshape([-1 if axis == axis_at else 1 for axis in range(len(shape))])
    return level


def gaussian(key, extent, deviation, most, cuts=(), kind=jnp.bfloat16):
    loudness = level_of(key, extent, cuts, -0.22, 0.18) if cuts else 1.0
    result = jax.random.normal(key, extent, jnp.float32) * deviation * loudness
    return jnp.minimum(jnp.maximum(result, -most), most).astype(kind)


def setup_inputs(seed: int = 0, part: int = 0) -> dict:
    key_list = jax.random.split(jax.random.key(seed), 14)
    part_keys = jax.random.split(jax.random.fold_in(key_list[13], part), 14)
    return {
        "query_nope": gaussian(part_keys[0], (TOKEN_COUNT, HEAD_COUNT * UNROTATED_SIZE), 2.5, 12.0, ((0, 4), (1, 4))),
        "query_rope": draw_query_rope(jax.random.fold_in(jax.random.fold_in(key_list[13], part), 71), part),
        "token_latent": gaussian(part_keys[2], (TOKEN_COUNT, LATENT_RANK), 1.0, 6.0, ((0, 4),)),
        "key_rope": draw_key_rope(jax.random.fold_in(jax.random.fold_in(key_list[13], part), 71), part),
        "latent_norm_gain": jnp.clip(1.0 + 0.18 * jax.random.normal(key_list[4], (LATENT_RANK,), jnp.float32), 0.1, 1.9),
        "key_expand_weight": gaussian(key_list[5], (LATENT_RANK, HEAD_COUNT * UNROTATED_SIZE), LATENT_RANK ** -0.5, 0.375),
        "value_expand_weight": gaussian(key_list[6], (LATENT_RANK, HEAD_COUNT * VALUE_SIZE), LATENT_RANK ** -0.5, 0.375),
        "residual": gaussian(part_keys[7], (TOKEN_COUNT, D), 0.5, 3.0, ((0, 4),)),
        "out_weight": gaussian(key_list[8], (HEAD_COUNT * VALUE_SIZE, D), (HEAD_COUNT * VALUE_SIZE // 4) ** -0.5, 0.375, ((0, 4),)),
        "ffn_gain": jnp.clip(1.0 + 0.18 * jax.random.normal(key_list[9], (D,), jnp.float32), 0.1, 1.9),
        "gate_weight": gaussian(key_list[10], (D, FF), D ** -0.5, 0.125, ((0, 4), (1, 4))),
        "up_weight": gaussian(key_list[11], (D, FF), D ** -0.5, 0.125, ((0, 4), (1, 4))),
        "down_weight": gaussian(key_list[12], (FF, D), FF ** -0.5, 0.078125, ((0, 4), (1, 4))),
    }


def norm_rows(values, gain):
    wide = values.astype(jnp.float32)
    return wide * lax.rsqrt(lax.optimization_barrier(jnp.mean(wide * wide, axis=-1, keepdims=True)) + 1e-06) * gain.astype(jnp.float32)

def turn_heads(vectors, positions):
    tokens, heads, width = vectors.shape
    freqs = width // 4
    grid_pos = jnp.stack([positions // GRID_W, positions % GRID_W], axis=-1).astype(jnp.float32)
    inverse = jnp.power(10000.0, -jnp.arange(freqs, dtype=jnp.float32) / freqs)
    angles = grid_pos[:, :, None] * inverse
    cosine = jnp.cos(angles)[:, None]
    sine = jnp.sin(angles)[:, None]
    viewed = vectors.reshape(tokens, heads, 2, 2, freqs)
    first = viewed[..., 0, :]
    second = viewed[..., 1, :]
    turned = jnp.stack([first * cosine - second * sine, first * sine + second * cosine], axis=-2)
    return turned.reshape(tokens, heads, width)

def reference(query_nope, query_rope, token_latent, key_rope, latent_norm_gain, key_expand_weight, value_expand_weight, residual, out_weight, ffn_gain, gate_weight, up_weight, down_weight):
    tokens = query_nope.shape[0]
    positions = jnp.arange(tokens, dtype=jnp.int32)
    query_flat = query_nope.reshape(tokens, HEAD_COUNT, UNROTATED_SIZE)
    query_turned = turn_heads(query_rope.astype(jnp.float32).reshape(tokens, HEAD_COUNT, ROPE), positions).astype(jnp.bfloat16)
    latent_normed = norm_rows(token_latent, latent_norm_gain).astype(jnp.bfloat16)
    key_turned = turn_heads(key_rope.astype(jnp.float32)[:, None, :], positions)[:, 0].astype(jnp.bfloat16)
    key_nope = jnp.dot(latent_normed, key_expand_weight, preferred_element_type=jnp.float32).astype(jnp.bfloat16)
    key_nope = key_nope.reshape(tokens, HEAD_COUNT, UNROTATED_SIZE)
    head_values = jnp.dot(latent_normed, value_expand_weight, preferred_element_type=jnp.float32).astype(jnp.bfloat16)
    head_values = head_values.reshape(tokens, HEAD_COUNT, VALUE_SIZE)
    score_scale = (UNROTATED_SIZE + ROPE) ** (-0.5)
    block_rows = math.gcd(tokens, 512)
    keys_wide = key_nope.astype(jnp.float32)
    rope_wide = key_turned.astype(jnp.float32)
    values_wide = head_values.astype(jnp.float32)

    def one_block(blocks):
        query_block, turned_block = blocks
        scores = (jnp.einsum('qhd,khd->hqk', query_block.astype(jnp.float32), keys_wide) + jnp.einsum('qhd,kd->hqk', turned_block.astype(jnp.float32), rope_wide)) * score_scale
        highest = lax.optimization_barrier(jnp.max(scores, axis=-1, keepdims=True))
        raised = jnp.exp(scores - highest)
        totals = lax.optimization_barrier(jnp.sum(raised, axis=-1))
        rounded = lax.optimization_barrier(raised.astype(jnp.bfloat16)).astype(jnp.float32)
        summed = jnp.einsum('hqk,khd->qhd', rounded, values_wide)
        return (summed / totals.T[:, :, None]).astype(jnp.bfloat16)
    attended = lax.map(one_block, (query_flat.reshape(-1, block_rows, HEAD_COUNT, UNROTATED_SIZE), query_turned.reshape(-1, block_rows, HEAD_COUNT, ROPE)))
    attended = attended.reshape(tokens, HEAD_COUNT * VALUE_SIZE)
    head_cols = HEAD_COUNT // N_TP * VALUE_SIZE
    mixed = residual.astype(jnp.float32)
    for member in range(N_TP):
        partial_out = jnp.dot(attended[:, member * head_cols:(member + 1) * head_cols], out_weight[member * head_cols:(member + 1) * head_cols], preferred_element_type=jnp.float32).astype(jnp.bfloat16)
        mixed = mixed + partial_out.astype(jnp.float32)
    normed = norm_rows(mixed, ffn_gain).astype(jnp.bfloat16)
    gate = jnp.dot(normed, gate_weight, preferred_element_type=jnp.float32)
    up_part = jnp.dot(normed, up_weight, preferred_element_type=jnp.float32)
    hidden = (jax.nn.silu(gate) * up_part).astype(jnp.bfloat16)
    hidden_cols = FF // N_TP
    layer_output = mixed
    for member in range(N_TP):
        partial_out = jnp.dot(hidden[:, member * hidden_cols:(member + 1) * hidden_cols], down_weight[member * hidden_cols:(member + 1) * hidden_cols], preferred_element_type=jnp.float32).astype(jnp.bfloat16)
        layer_output = layer_output + partial_out.astype(jnp.float32)
    return layer_output.astype(jnp.bfloat16)
```

```python
import functools

import jax
import jax.numpy as jnp
import numpy as np
from jax import lax
from jax.experimental import pallas as pl
from jax.experimental.pallas import tpu as pltpu
from jax.sharding import PartitionSpec as P

MESH = pl.DeviceIdType.MESH
UNROTATED_SIZE = 64
ROPE = 32
VALUE_SIZE = 64
GRID_W = 64


def norm_rows(values, gain):
    wide = values.astype(jnp.float32)
    return wide * lax.rsqrt(jnp.mean(wide * wide, axis=-1, keepdims=True) + 1e-06) * gain


def turn_heads(vectors, positions):
    tokens, heads, width = vectors.shape
    freqs = width // 4
    grid_pos = jnp.stack([positions // GRID_W, positions % GRID_W], axis=-1).astype(jnp.float32)
    inverse = jnp.power(10000.0, -jnp.arange(freqs, dtype=jnp.float32) / freqs)
    angles = grid_pos[:, :, None] * inverse
    cosine = jnp.cos(angles)[:, None]
    sine = jnp.sin(angles)[:, None]
    viewed = vectors.reshape(tokens, heads, 2, 2, freqs)
    first = viewed[..., 0, :]
    second = viewed[..., 1, :]
    turned = jnp.stack([first * cosine - second * sine, first * sine + second * cosine], axis=-2)
    return turned.reshape(tokens, heads, width)


def spread_hidden(token_count, hidden_columns):
    fits = lax.axis_size("tp") == 4 and lax.axis_size("grp") == 2
    return fits and 2 * token_count < 3 * hidden_columns


def column_tiles(hidden_columns):
    tiles = hidden_columns // 128
    return tiles, -(-tiles // lax.axis_size("sp"))


def window_start(at, hidden_columns):
    tiles, per = column_tiles(hidden_columns)
    return lax.div(at * (tiles - per), lax.axis_size("sp") - 1)


def signal_all(peers):
    barrier = pltpu.get_barrier_semaphore()
    for peer in peers:
        pl.semaphore_signal(barrier, inc=1, device_id=peer, device_id_type=MESH)
    pl.semaphore_wait(barrier, len(peers))


def remote(src, dst, send_sem, recv_sem, peer):
    return pltpu.make_async_remote_copy(
        src_ref=src,
        dst_ref=dst,
        send_sem=send_sem,
        recv_sem=recv_sem,
        device_id=peer,
        device_id_type=MESH,
    )


def line_order(here, size):
    table = []
    for at in range(size):
        others = [place for place in range(size) if place != at]
        flip = 1 if 2 * at < size else -1
        table.append(sorted(others, key=lambda place: (abs(place - at), (place - at) * flip)))
    columns = []
    for step in range(size - 1):
        value = jnp.int32(0)
        for at in range(size):
            value = value + jnp.where(here == at, table[at][step], 0)
        columns.append(value)
    return columns


def swap_matrix(lanes):
    freqs = ROPE // 4
    row = lax.broadcasted_iota(jnp.int32, (lanes, lanes), 0)
    lane = lax.broadcasted_iota(jnp.int32, (lanes, lanes), 1)
    first_half = lax.rem(lane, 2 * freqs) < freqs
    partner = jnp.where(first_half, lane + freqs, lane - freqs)
    sign = jnp.where(first_half, -1.0, 1.0)
    return jnp.where(row == partner, sign, 0.0).astype(jnp.bfloat16)


def layer_kernel(
    size, hidden_columns, query, query_rope, token_latent, key_rope, latent_gain, table,
    key_w, value_w, out_w, residual, gain, gate, up, down,
    out,
    gathered, keys, values, gate_v, up_v, down_v, projected, p_core, p_x,
    tokens, parts, from_core, from_x, from_z, total,
    own_sem, w_send, w_recv, y_send, y_recv,
    lz_send, lz_recv, lx_send, lx_recv, lc_send, lc_recv,
    pc_send, pc_recv, px_send, px_recv,
    z_send, z_recv, x_send, x_recv, c_send, c_recv,
    rc_send, rc_recv, rx_send, rx_recv, rz_send, rz_recv,
):
    here = lax.axis_index("sp")
    part = lax.axis_index("grp")
    t = lax.axis_index("tp")
    core = t + 1 - 2 * lax.rem(t, 2)
    across = t + 2 - 4 * lax.div(t, 2)
    diagonal = core + 2 - 4 * lax.div(core, 2)
    to_core, to_x = {"tp": core}, {"tp": across}
    depth = gate.shape[0]
    width = gate_v.shape[1]
    outer = down.shape[1]
    count = token_latent.shape[0]
    rank = token_latent.shape[1]
    rows = count // 4
    model = residual.shape[1]
    order = line_order(here, size)
    origins = [here] + order
    last = size - 1
    pending = []

    def start(*args):
        copy = remote(*args)
        copy.start()
        pending.append(copy)
        return copy

    def start_of(at):
        return pl.multiple_of(window_start(at, hidden_columns) * 128, 128)

    def piece(ref, kind, origin, half):
        if kind < 2:
            step = depth // 2
            return ref.at[pl.ds(pl.multiple_of(origin * depth + half * step, step), step), :]
        step = width // 2
        return ref.at[
            pl.ds(pl.multiple_of(half * step, step), step),
            pl.ds(pl.multiple_of(origin * outer, outer), outer),
        ]

    def source(ref, kind, target, half):
        if kind < 2:
            step = depth // 2
            return ref.at[pl.ds(pl.multiple_of(half * step, step), step), pl.ds(start_of(target), width)]
        step = width // 2
        return ref.at[pl.ds(pl.multiple_of(start_of(target) + half * step, 64), step), :]

    rope_own = key_rope[...]
    repeats = query_rope.shape[1] // ROPE
    gathered[here, :, :rank] = token_latent[...]
    gathered[here, :, rank:] = jnp.concatenate([rope_own] * repeats, axis=1)

    peers = [{"sp": lax.rem(here + shift, size)} for shift in range(1, size)]
    signal_all(peers + [to_core, to_x, {"grp": 1 - part}])

    def quarter(at):
        return pl.ds(pl.multiple_of(at * rows, rows), rows)

    lz = []
    for shift in range(1, size):
        held = gathered.at[here, quarter(t), :]
        lz.append(
            start(held, held, lz_send.at[shift - 1], lz_recv.at[shift - 1], {"sp": lax.rem(here + shift, size)})
        )
    refs = ((gate, gate_v), (up, up_v), (down, down_v))
    crossing = [[], [], []]

    def spread(kind):
        ref, held = refs[kind]
        for shift in range(1, size):
            target = lax.rem(here + shift, size)
            crossing[kind].append(
                start(
                    source(ref, kind, target, part),
                    piece(held, kind, here, part),
                    w_send.at[kind, shift - 1],
                    w_recv.at[kind, shift - 1],
                    {"sp": target},
                )
            )

    spread(0)
    spread(1)
    spread(2)
    locals_ = [[], [], []]
    for kind, (ref, held) in enumerate(refs):
        for half in range(2):
            copy = pltpu.make_async_copy(
                source(ref, kind, here, half), piece(held, kind, here, half), own_sem.at[kind, half]
            )
            copy.start()
            locals_[kind].append(copy)

    lanes = query.shape[1]
    heads = lanes // UNROTATED_SIZE
    columns = pl.ds(pl.multiple_of(t * lanes, 128), lanes)
    swap = swap_matrix(query_rope.shape[1])

    def turn(vectors, first):
        where = pl.ds(pl.multiple_of(first, 8), vectors.shape[0])
        other = jnp.dot(vectors, swap, preferred_element_type=jnp.float32)
        turned = vectors.astype(jnp.float32) * table[0, where, :] + other * table[1, where, :]
        return turned.astype(jnp.bfloat16)

    def expand(origin):
        where = pl.ds(pl.multiple_of(origin * count, count), count)
        latent = norm_rows(gathered[origin, :, :rank], latent_gain[...]).astype(jnp.bfloat16)
        keys[where, :lanes] = jnp.dot(
            latent, key_w[:, columns], preferred_element_type=jnp.float32
        ).astype(jnp.bfloat16)
        keys[where, lanes:] = turn(gathered[origin, :, rank:], origin * count)
        values[where, :] = jnp.dot(
            latent, value_w[:, columns], preferred_element_type=jnp.float32
        ).astype(jnp.bfloat16)

    turned = turn(query_rope[...], here * count)
    expand(here)
    lx, lc = {}, {}
    for shift in range(1, size):
        origin = lax.rem(here - shift + size, size)
        lz[shift - 1].wait_recv()
        held = gathered.at[origin, quarter(t), :]
        lx[shift] = start(held, held, lx_send.at[shift - 1], lx_recv.at[shift - 1], to_x)
        lc[shift] = start(held, held, lc_send.at[shift - 1, 0], lc_recv.at[shift - 1, 0], to_core)
    lc_second = {}
    for shift in range(1, size):
        origin = lax.rem(here - shift + size, size)
        lx[shift].wait_recv()
        held = gathered.at[origin, quarter(across), :]
        lc_second[shift] = start(held, held, lc_send.at[shift - 1, 1], lc_recv.at[shift - 1, 1], to_core)
    for shift in range(1, size):
        lc[shift].wait_recv()
        lc_second[shift].wait_recv()
        expand(lax.rem(here - shift + size, size))

    scale = (UNROTATED_SIZE + ROPE) ** (-0.5)
    lane = lax.broadcasted_iota(jnp.int32, (1, lanes), 1)
    rope_lane = lax.broadcasted_iota(jnp.int32, (1, turned.shape[1]), 1)
    attended = jnp.zeros((count, lanes), jnp.float32)
    for head in range(heads):
        mine = (lane >= head * UNROTATED_SIZE) & (lane < (head + 1) * UNROTATED_SIZE)
        rope_mine = (rope_lane >= head * ROPE) & (rope_lane < (head + 1) * ROPE)
        both = jnp.concatenate(
            [
                jnp.where(mine, query[...].astype(jnp.float32), 0.0),
                jnp.where(rope_mine, turned.astype(jnp.float32), 0.0),
            ],
            axis=1,
        ).astype(jnp.bfloat16)
        scores = (
            lax.dot_general(
                both, keys[...], (((1,), (1,)), ((), ())), preferred_element_type=jnp.float32
            )
            * scale
        )
        raised = jnp.exp(scores - jnp.max(scores, axis=1, keepdims=True))
        totals = jnp.sum(raised, axis=1, keepdims=True)
        weighted = jnp.dot(
            raised.astype(jnp.bfloat16), values[...], preferred_element_type=jnp.float32
        )
        attended = jnp.where(mine, weighted / totals, attended)
    attended = attended.astype(jnp.bfloat16)
    step = 512
    for col in range(0, model, step):
        term = jnp.dot(attended, out_w[:, col : col + step], preferred_element_type=jnp.float32)
        projected[:, :, col : col + step] = term.astype(jnp.bfloat16).reshape(4, rows, step)

    def plus(one, two):
        return one.astype(jnp.float32) + two.astype(jnp.float32)

    pc_first = start(projected.at[diagonal], p_core.at[1], pc_send.at[1], pc_recv.at[1], to_core)
    pc_second = start(projected.at[core], p_core.at[0], pc_send.at[0], pc_recv.at[0], to_core)
    pc_first.wait_recv()
    projected[across] = plus(projected[across], p_core[1]).astype(jnp.bfloat16)
    px = start(projected.at[across], p_x, px_send, px_recv, to_x)

    swaps = [[], [], []]

    def forward(kind):
        held_ref = refs[kind][1]
        for shift in range(1, size):
            origin = lax.rem(here - shift + size, size)
            crossing[kind][shift - 1].wait_recv()
            held = piece(held_ref, kind, origin, part)
            swaps[kind].append(
                start(held, held, y_send.at[kind, shift - 1], y_recv.at[kind, shift - 1], {"grp": 1 - part})
            )

    def settle(kind):
        for copy in locals_[kind]:
            copy.wait()
        for copy in swaps[kind]:
            copy.wait_recv()

    pc_second.wait_recv()
    total[...] = residual[quarter(t), :].astype(jnp.float32) + plus(projected[t], p_core[0])
    forward(0)
    px.wait_recv()
    mixed = total[...] + p_x[...].astype(jnp.float32)
    total[...] = mixed
    tokens[here, t] = (
        mixed * lax.rsqrt(jnp.mean(mixed * mixed, axis=1, keepdims=True) + 1e-06) * gain[...]
    ).astype(jnp.bfloat16)

    own_block = tokens.at[here, t]

    def own_copy(way):
        target = here + 1 - 2 * way
        return remote(own_block, own_block, z_send.at[way], z_recv.at[here], {"sp": target})

    @pl.when(here < last)
    def _():
        own_copy(0).start()

    @pl.when(here > 0)
    def _():
        own_copy(1).start()

    def passing(i):
        origin = origins[i]
        block = tokens.at[origin, t]
        target = jnp.where(origin < here, here + 1, here - 1)
        valid = (target >= 0) & (target <= last)
        target = jnp.clip(target, 0, last)
        return valid, remote(block, block, z_send.at[1 + i], z_recv.at[origin], {"sp": target})

    x_copies, c_first, c_second, r_first, r_second, rx, rz = {}, {}, {}, {}, {}, {}, {}

    def step_a(i):
        o = origins[i]
        block = tokens.at[o, t]
        if i:
            remote(block, block, z_send.at[1 + i], z_recv.at[o], to_x).wait_recv()
            valid, copy = passing(i)
            pl.when(valid)(copy.start)
        x_copies[i] = start(block, block, x_send.at[i], x_recv.at[i], to_x)
        c_first[i] = start(block, block, c_send.at[i, 0], c_recv.at[i, 0], to_core)

    def step_b(i):
        x_copies[i].wait_recv()
        block = tokens.at[origins[i], across]
        c_second[i] = start(block, block, c_send.at[i, 1], c_recv.at[i, 1], to_core)

    tiles, per = column_tiles(hidden_columns)
    before = jnp.where(here > 0, window_start(jnp.maximum(here - 1, 0), hidden_columns) + per, 0)
    first = (before - window_start(here, hidden_columns)) * 128
    keep = lax.broadcasted_iota(jnp.int32, (1, width), 1) >= first

    def step_c(i):
        o = origins[i]
        c_first[i].wait_recv()
        c_second[i].wait_recv()
        if i == 0:
            settle(0)
            settle(1)
        x = tokens[o].reshape(4 * rows, model)
        gated = jnp.dot(x, gate_v[...], preferred_element_type=jnp.float32)
        lifted = jnp.dot(x, up_v[...], preferred_element_type=jnp.float32)
        hidden = jnp.where(keep, gated / (1.0 + jnp.exp(-gated)) * lifted, 0.0).astype(jnp.bfloat16)
        if i == 0:
            forward(2)
            settle(2)
        for col in range(0, model, step):
            term = jnp.dot(hidden, down_v[:, col : col + step], preferred_element_type=jnp.float32)
            parts[o, :, :, col : col + step] = term.astype(jnp.bfloat16).reshape(4, rows, step)
        r_first[i] = start(parts.at[o, diagonal], from_core.at[i, 1], rc_send.at[i, 1], rc_recv.at[i, 1], to_core)
        r_second[i] = start(parts.at[o, core], from_core.at[i, 0], rc_send.at[i, 0], rc_recv.at[i, 0], to_core)

    def step_d(i):
        o = origins[i]
        r_first[i].wait_recv()
        parts[o, across] = plus(parts[o, across], from_core[i, 1]).astype(jnp.bfloat16)
        rx[i] = start(parts.at[o, across], from_x.at[i], rx_send.at[i], rx_recv.at[i], to_x)
        r_second[i].wait_recv()
        parts[o, t] = plus(parts[o, t], from_core[i, 0]).astype(jnp.bfloat16)

    def step_e(i):
        o = origins[i]
        rx[i].wait_recv()
        if i == 0:
            total[...] = total[...] + plus(parts[o, t], from_x[i])
            return
        parts[o, t] = plus(parts[o, t], from_x[i]).astype(jnp.bfloat16)
        rz[i] = start(parts.at[o, t], from_z.at[here], rz_send.at[i], rz_recv.at[here], {"sp": o})

    steps = {"a": step_a, "b": step_b, "c": step_c, "d": step_d, "e": step_e}
    step_a(0)
    forward(1)
    sequence = []
    for i in range(size + 1):
        for name, lag in (("a", -1), ("b", 0), ("c", 0), ("d", 0), ("e", 1)):
            if 0 <= i - lag <= last and (name, i - lag) != ("a", 0):
                sequence.append((name, i - lag))
    for name, i in sequence:
        steps[name](i)
    result = total[...]
    for i in range(1, size):
        o = origins[i]
        remote(from_z.at[o], from_z.at[o], rz_send.at[i], rz_recv.at[o], to_x).wait_recv()
        result = result + from_z[o].astype(jnp.float32)
    out[...] = result.astype(out.dtype)

    @pl.when(here < last)
    def _():
        own_copy(0).wait_send()

    @pl.when(here > 0)
    def _():
        own_copy(1).wait_send()

    for i in range(1, size):
        valid, copy = passing(i)
        pl.when(valid)(copy.wait_send)
    for copy in pending:
        copy.wait_send()


def position_table(token_count, lanes):
    freqs = ROPE // 4
    lane = np.arange(lanes)
    place = np.arange(token_count)
    inverse = np.power(10000.0, -(lane % freqs).astype(np.float64) / freqs)
    grid = np.where((lane % ROPE < ROPE // 2)[None], (place // GRID_W)[:, None], (place % GRID_W)[:, None])
    angles = grid.astype(np.float64) * inverse[None]
    return np.stack([np.cos(angles), np.sin(angles)]).astype(np.float32)


def spread_layer(
    query_nope, query_rope, token_latent, key_rope, latent_norm_gain, key_w, value_w,
    residual, out_w, ffn_gain, gate_w, up_w, down_w,
):
    size = lax.axis_size("sp")
    depth, columns = gate_w.shape
    width = column_tiles(columns)[1] * 128
    count, model = residual.shape
    lanes = query_nope.shape[1]
    wide = token_latent.shape[1] + query_rope.shape[1]
    block = (count // 4, model)
    table = jnp.asarray(position_table(size * count, query_rope.shape[1]))
    dma = pltpu.SemaphoreType.DMA
    narrow = jnp.bfloat16
    vmem = lambda *lead: pltpu.VMEM(lead + block, narrow)
    line = [dma((size - 1,)), dma((size - 1,))]
    line_pair = [dma((size - 1, 2)), dma((size - 1, 2))]
    pieces = [dma((3, size - 1)), dma((3, size - 1))]
    single = [dma((size,)), dma((size,))]
    double = [dma((size, 2)), dma((size, 2))]
    here = pl.BlockSpec(memory_space=pltpu.VMEM)
    away = pl.BlockSpec(memory_space=pl.ANY)
    return pl.pallas_call(
        functools.partial(layer_kernel, size, columns),
        out_shape=jax.ShapeDtypeStruct(block, narrow),
        in_specs=[here] * 11 + [away] * 3,
        out_specs=here,
        scratch_shapes=[
            pltpu.VMEM((size, count, wide), narrow),
            pltpu.VMEM((size * count, lanes + query_rope.shape[1]), narrow),
            pltpu.VMEM((size * count, lanes), narrow),
            pltpu.VMEM((size * depth, width), narrow),
            pltpu.VMEM((size * depth, width), narrow),
            pltpu.VMEM((width, size * down_w.shape[1]), narrow),
            vmem(4), vmem(2), vmem(),
            vmem(size, 4), vmem(size, 4), vmem(size, 2), vmem(size), vmem(size),
            pltpu.VMEM(block, jnp.float32),
            dma((3, 2)), *pieces, *pieces,
            *line, *line, *line_pair,
            dma((2,)), dma((2,)), dma, dma,
            dma((size + 1,)), dma((size,)), *single, *double, *double, *single, *single,
        ],
        compiler_params=pltpu.CompilerParams(collective_id=0, has_side_effects=True),
        name="layer",
    )(
        query_nope, query_rope, token_latent, key_rope, latent_norm_gain[None], table,
        key_w, value_w, out_w, residual, ffn_gain[None], gate_w, up_w, down_w,
    )


def local(
    query_nope,
    query_rope,
    token_latent,
    key_rope,
    latent_norm_gain,
    key_expand_weight,
    value_expand_weight,
    residual,
    out_weight,
    ffn_gain,
    gate_weight,
    up_weight,
    down_weight,
):
    if spread_hidden(query_nope.shape[0] * lax.axis_size("sp"), gate_weight.shape[1]):
        return spread_layer(
            query_nope,
            query_rope,
            token_latent,
            key_rope,
            latent_norm_gain,
            key_expand_weight,
            value_expand_weight,
            residual,
            out_weight,
            ffn_gain,
            gate_weight,
            up_weight,
            down_weight,
        )
    tok_rows = query_nope.shape[0]
    heads_here = query_nope.shape[1] // UNROTATED_SIZE
    own_rows = tok_rows // lax.axis_size("tp")
    tp_index = lax.axis_index("tp")
    positions = lax.axis_index("sp") * tok_rows + jnp.arange(tok_rows, dtype=jnp.int32)
    query_flat = query_nope.reshape(tok_rows, heads_here, UNROTATED_SIZE)
    query_turned = turn_heads(
        query_rope.astype(jnp.float32).reshape(tok_rows, heads_here, ROPE), positions
    ).astype(jnp.bfloat16)
    latent = norm_rows(token_latent, latent_norm_gain).astype(jnp.bfloat16)
    key_turned = turn_heads(key_rope.astype(jnp.float32)[:, None, :], positions)[:, 0].astype(
        jnp.bfloat16
    )
    key_cols = lax.dynamic_slice_in_dim(
        key_expand_weight, tp_index * heads_here * UNROTATED_SIZE, heads_here * UNROTATED_SIZE, 1
    )
    value_cols = lax.dynamic_slice_in_dim(
        value_expand_weight, tp_index * heads_here * VALUE_SIZE, heads_here * VALUE_SIZE, 1
    )
    score_scale = (UNROTATED_SIZE + ROPE) ** (-0.5)

    def absorb(carried, block_in):
        latent_block, rope_block = block_in
        block_rows = latent_block.shape[0]
        key_rows = jnp.dot(latent_block, key_cols, preferred_element_type=jnp.float32).astype(
            jnp.bfloat16
        )
        key_rows = key_rows.reshape(block_rows, heads_here, UNROTATED_SIZE)
        value_rows = jnp.dot(latent_block, value_cols, preferred_element_type=jnp.float32).astype(
            jnp.bfloat16
        )
        value_rows = value_rows.reshape(block_rows, heads_here, VALUE_SIZE)
        scores = (
            jnp.einsum("qhd,khd->hqk", query_flat, key_rows, preferred_element_type=jnp.float32)
            + jnp.einsum(
                "qhd,kd->hqk", query_turned, rope_block, preferred_element_type=jnp.float32
            )
        ) * score_scale
        highest, totals, accumulated = carried
        new_highest = jnp.maximum(highest, jnp.max(scores, axis=-1))
        shrink = jnp.exp(highest - new_highest)
        weights = jnp.exp(scores - new_highest[:, :, None])
        totals = totals * shrink + jnp.sum(weights, axis=-1)
        accumulated = accumulated * shrink.T[:, :, None] + jnp.einsum(
            "hqk,khd->qhd",
            weights.astype(jnp.bfloat16),
            value_rows,
            preferred_element_type=jnp.float32,
        )
        return ((new_highest, totals, accumulated), None)

    initial = (
        jnp.full((heads_here, tok_rows), -jnp.inf, jnp.float32),
        jnp.zeros((heads_here, tok_rows), jnp.float32),
        jnp.zeros((tok_rows, heads_here, VALUE_SIZE), jnp.float32),
    )
    carried = initial
    latent_piece = lax.all_gather(latent, "sp", axis=0, tiled=True)
    rope_piece = lax.all_gather(key_turned, "sp", axis=0, tiled=True)
    shard_count = latent_piece.shape[0] // tok_rows
    grouped = max(
        (
            factor
            for factor in range(1, shard_count + 1)
            if shard_count % factor == 0 and factor * tok_rows <= max(1024, tok_rows)
        )
    )
    block_rows = grouped * tok_rows
    blocks = (
        latent_piece.reshape(-1, block_rows, latent_piece.shape[1]),
        rope_piece.reshape(-1, block_rows, rope_piece.shape[1]),
    )
    carried, _ = lax.scan(absorb, carried, blocks)
    highest, totals, accumulated = carried
    attended = (
        (accumulated / totals.T[:, :, None])
        .reshape(tok_rows, heads_here * VALUE_SIZE)
        .astype(jnp.bfloat16)
    )
    projected = jnp.dot(attended, out_weight, preferred_element_type=jnp.float32).astype(
        jnp.bfloat16
    )
    summed = lax.psum(projected, "tp").astype(jnp.float32)
    mixed_all = residual.astype(jnp.float32) + summed
    normed_all = norm_rows(mixed_all, ffn_gain).astype(jnp.bfloat16)
    mixed_own = lax.dynamic_slice_in_dim(mixed_all, tp_index * own_rows, own_rows, 0)
    gate_piece = lax.all_gather(gate_weight, "sp", axis=0, tiled=True)
    up_piece = lax.all_gather(up_weight, "sp", axis=0, tiled=True)
    gate = jnp.dot(normed_all, gate_piece, preferred_element_type=jnp.float32)
    up_part = jnp.dot(normed_all, up_piece, preferred_element_type=jnp.float32)
    hidden = (jax.nn.silu(gate) * up_part).astype(jnp.bfloat16)
    terms = jnp.dot(
        hidden,
        lax.all_gather(down_weight, "sp", axis=1, tiled=True),
        preferred_element_type=jnp.float32,
    )
    ffn_own = lax.psum_scatter(
        terms.astype(jnp.bfloat16), "tp", scatter_dimension=0, tiled=True
    ).astype(jnp.float32)
    return (mixed_own + ffn_own).astype(jnp.bfloat16)


def solution(mesh):
    return jax.shard_map(
        local,
        mesh=mesh,
        in_specs=(
            P(("grp", "sp"), "tp"),
            P(("grp", "sp"), "tp"),
            P(("grp", "sp"), None),
            P(("grp", "sp"), None),
            P(),
            P(),
            P(),
            P(("grp", "sp"), None),
            P("tp", None),
            P(),
            P("sp", "tp"),
            P("sp", "tp"),
            P("tp", "sp"),
        ),
        out_specs=P(("grp", "sp", "tp"), None),
        check_vma=False,
    )
```

```python
import functools

import jax
import jax.numpy as jnp
import numpy as np
from jax import lax
from jax.experimental import pallas as pl
from jax.experimental.pallas import tpu as pltpu
from jax.sharding import PartitionSpec as P

MESH = pl.DeviceIdType.MESH
UNROTATED_SIZE = 64
ROPE = 32
VALUE_SIZE = 64
GRID_W = 64


def norm_rows(values, gain):
    wide = values.astype(jnp.float32)
    return wide * lax.rsqrt(jnp.mean(wide * wide, axis=-1, keepdims=True) + 1e-06) * gain


def turn_heads(vectors, positions):
    tokens, heads, width = vectors.shape
    freqs = width // 4
    grid_pos = jnp.stack([positions // GRID_W, positions % GRID_W], axis=-1).astype(jnp.float32)
    inverse = jnp.power(10000.0, -jnp.arange(freqs, dtype=jnp.float32) / freqs)
    angles = grid_pos[:, :, None] * inverse
    cosine = jnp.cos(angles)[:, None]
    sine = jnp.sin(angles)[:, None]
    viewed = vectors.reshape(tokens, heads, 2, 2, freqs)
    first = viewed[..., 0, :]
    second = viewed[..., 1, :]
    turned = jnp.stack([first * cosine - second * sine, first * sine + second * cosine], axis=-2)
    return turned.reshape(tokens, heads, width)


def spread_hidden(token_count, hidden_columns):
    fits = lax.axis_size("tp") == 4 and lax.axis_size("grp") == 2
    return fits and 2 * token_count < 3 * hidden_columns


def column_tiles(hidden_columns):
    tiles = hidden_columns // 128
    return tiles, -(-tiles // lax.axis_size("sp"))


def window_start(at, hidden_columns):
    tiles, per = column_tiles(hidden_columns)
    return lax.div(at * (tiles - per), lax.axis_size("sp") - 1)


def signal_all(peers):
    barrier = pltpu.get_barrier_semaphore()
    for peer in peers:
        pl.semaphore_signal(barrier, inc=1, device_id=peer, device_id_type=MESH)
    pl.semaphore_wait(barrier, len(peers))


def remote(src, dst, send_sem, recv_sem, peer):
    return pltpu.make_async_remote_copy(
        src_ref=src,
        dst_ref=dst,
        send_sem=send_sem,
        recv_sem=recv_sem,
        device_id=peer,
        device_id_type=MESH,
    )


def line_order(here, size):
    table = []
    for at in range(size):
        others = [place for place in range(size) if place != at]
        flip = 1 if 2 * at < size else -1
        table.append(sorted(others, key=lambda place: (abs(place - at), (place - at) * flip)))
    columns = []
    for step in range(size - 1):
        value = jnp.int32(0)
        for at in range(size):
            value = value + jnp.where(here == at, table[at][step], 0)
        columns.append(value)
    return columns


def swap_matrix(lanes):
    freqs = ROPE // 4
    row = lax.broadcasted_iota(jnp.int32, (lanes, lanes), 0)
    lane = lax.broadcasted_iota(jnp.int32, (lanes, lanes), 1)
    first_half = lax.rem(lane, 2 * freqs) < freqs
    partner = jnp.where(first_half, lane + freqs, lane - freqs)
    sign = jnp.where(first_half, -1.0, 1.0)
    return jnp.where(row == partner, sign, 0.0).astype(jnp.bfloat16)


def layer_kernel(
    size, hidden_columns, query, query_rope, token_latent, key_rope, latent_gain,
    key_all, value_all, out_all, residual_all, table_all, gain, gate, up, down,
    out,
    key_w, value_w, out_w, residual, table, gathered, keys, values, gate_v, up_v, down_v, projected, p_core, p_x,
    tokens, parts, hidden, from_core, from_x, from_z, total,
    in_sem, own_sem, w_send, w_recv, y_send, y_recv,
    lz_send, lz_recv, lx_send, lx_recv, lc_send, lc_recv,
    pc_send, pc_recv, px_send, px_recv,
    z_send, z_recv, x_send, x_recv, c_send, c_recv,
    rc_send, rc_recv, rx_send, rx_recv, rz_send, rz_recv,
):
    here = lax.axis_index("sp")
    part = lax.axis_index("grp")
    t = lax.axis_index("tp")
    core = t + 1 - 2 * lax.rem(t, 2)
    across = t + 2 - 4 * lax.div(t, 2)
    diagonal = core + 2 - 4 * lax.div(core, 2)
    to_core, to_x = {"tp": core}, {"tp": across}
    depth = gate.shape[0]
    width = gate_v.shape[1]
    outer = down.shape[1]
    count = token_latent.shape[0]
    rank = token_latent.shape[1]
    rows = count // 4
    model = residual.shape[1]
    lanes = query.shape[1]
    columns = pl.ds(pl.multiple_of(t * lanes, 128), lanes)
    step = outer
    order = line_order(here, size)
    origins = [here] + order
    last = size - 1
    pending = []

    def start(*args):
        copy = remote(*args)
        copy.start()
        pending.append(copy)
        return copy

    def start_of(at):
        return pl.multiple_of(window_start(at, hidden_columns) * 128, 128)

    def piece(ref, kind, origin, half):
        if kind < 2:
            step = depth // 2
            return ref.at[pl.ds(pl.multiple_of(origin * depth + half * step, step), step), :]
        step = width // 2
        return ref.at[
            pl.ds(pl.multiple_of(half * step, step), step),
            pl.ds(pl.multiple_of(origin * outer, outer), outer),
        ]

    def source(ref, kind, target, half):
        if kind < 2:
            step = depth // 2
            return ref.at[pl.ds(pl.multiple_of(half * step, step), step), pl.ds(start_of(target), width)]
        step = width // 2
        return ref.at[pl.ds(pl.multiple_of(start_of(target) + half * step, 64), step), :]

    def quarter(at):
        return pl.ds(pl.multiple_of(at * rows, rows), rows)

    loads = [
        pltpu.make_async_copy(src, dst, in_sem.at[n])
        for n, (src, dst) in enumerate(
            (
                (table_all, table),
                (key_all.at[:, columns], key_w),
                (value_all.at[:, columns], value_w),
                (out_all, out_w),
                (residual_all.at[quarter(t), :], residual),
            )
        )
    ]
    for copy in loads:
        copy.start()
    rope_own = key_rope[...]
    repeats = query_rope.shape[1] // ROPE
    gathered[here, :, :rank] = token_latent[...]
    gathered[here, :, rank:] = jnp.concatenate([rope_own] * repeats, axis=1)

    peers = [{"sp": lax.rem(here + shift, size)} for shift in range(1, size)]
    with jax.named_scope('barrier'):
        signal_all(peers + [to_core, to_x, {"grp": 1 - part}])

    lz = []
    for shift in range(1, size):
        held = gathered.at[here, quarter(t), :]
        lz.append(
            start(held, held, lz_send.at[shift - 1], lz_recv.at[shift - 1], {"sp": lax.rem(here + shift, size)})
        )
    refs = ((gate, gate_v), (up, up_v), (down, down_v))
    crossing = [[], [], []]

    def spread(kind):
        ref, held = refs[kind]
        for shift in range(1, size):
            target = lax.rem(here + shift, size)
            crossing[kind].append(
                start(
                    source(ref, kind, target, part),
                    piece(held, kind, here, part),
                    w_send.at[kind, shift - 1],
                    w_recv.at[kind, shift - 1],
                    {"sp": target},
                )
            )

    locals_ = [[], [], []]
    for kind, (ref, held) in enumerate(refs):
        for half in range(2):
            copy = pltpu.make_async_copy(
                source(ref, kind, here, half), piece(held, kind, here, half), own_sem.at[kind, half]
            )
            copy.start()
            locals_[kind].append(copy)

    heads = lanes // UNROTATED_SIZE
    swap = swap_matrix(query_rope.shape[1])

    def turn(vectors, first):
        where = pl.ds(pl.multiple_of(first, 8), vectors.shape[0])
        other = jnp.dot(vectors, swap, preferred_element_type=jnp.float32)
        turned = vectors.astype(jnp.float32) * table[0, where, :] + other * table[1, where, :]
        return turned.astype(jnp.bfloat16)

    def expand(origin):
        where = pl.ds(pl.multiple_of(origin * count, count), count)
        latent = norm_rows(gathered[origin, :, :rank], latent_gain[...]).astype(jnp.bfloat16)
        keys[where, :lanes] = jnp.dot(
            latent, key_w[...], preferred_element_type=jnp.float32
        ).astype(jnp.bfloat16)
        keys[where, lanes:] = turn(gathered[origin, :, rank:], origin * count)
        values[where, :] = jnp.dot(
            latent, value_w[...], preferred_element_type=jnp.float32
        ).astype(jnp.bfloat16)

    for copy in loads[:3]:
        copy.wait()
    with jax.named_scope('own_kv'):
        turned = turn(query_rope[...], here * count)
        expand(here)
    lx, lc = {}, {}
    for shift in range(1, size):
        origin = lax.rem(here - shift + size, size)
        with jax.named_scope('lat_z'):
            lz[shift - 1].wait_recv()
        held = gathered.at[origin, quarter(t), :]
        lx[shift] = start(held, held, lx_send.at[shift - 1], lx_recv.at[shift - 1], to_x)
        lc[shift] = start(held, held, lc_send.at[shift - 1, 0], lc_recv.at[shift - 1, 0], to_core)
    spread(0)
    spread(1)
    lc_second = {}
    for shift in range(1, size):
        origin = lax.rem(here - shift + size, size)
        with jax.named_scope('lat_x'):
            lx[shift].wait_recv()
        held = gathered.at[origin, quarter(across), :]
        lc_second[shift] = start(held, held, lc_send.at[shift - 1, 1], lc_recv.at[shift - 1, 1], to_core)
    for shift in range(1, size):
        lc[shift].wait_recv()
        with jax.named_scope('lat_c'):
            lc_second[shift].wait_recv()
        with jax.named_scope('expand'):
            expand(lax.rem(here - shift + size, size))

    scale = (UNROTATED_SIZE + ROPE) ** (-0.5)
    lane = lax.broadcasted_iota(jnp.int32, (1, lanes), 1)
    rope_lane = lax.broadcasted_iota(jnp.int32, (1, turned.shape[1]), 1)
    attended = jnp.zeros((count, lanes), jnp.float32)
    with jax.named_scope('heads'):
        for head in range(heads):
            mine = (lane >= head * UNROTATED_SIZE) & (lane < (head + 1) * UNROTATED_SIZE)
            rope_mine = (rope_lane >= head * ROPE) & (rope_lane < (head + 1) * ROPE)
            both = jnp.concatenate(
                [
                    jnp.where(mine, query[...].astype(jnp.float32), 0.0),
                    jnp.where(rope_mine, turned.astype(jnp.float32), 0.0),
                ],
                axis=1,
            ).astype(jnp.bfloat16)
            scores = (
                lax.dot_general(
                    both, keys[...], (((1,), (1,)), ((), ())), preferred_element_type=jnp.float32
                )
                * scale
            )
            raised = jnp.exp(scores - jnp.max(scores, axis=1, keepdims=True))
            totals = jnp.sum(raised, axis=1, keepdims=True)
            weighted = jnp.dot(
                raised.astype(jnp.bfloat16), values[...], preferred_element_type=jnp.float32
            )
            attended = jnp.where(mine, weighted / totals, attended)
    attended = attended.astype(jnp.bfloat16)
    for copy in loads[3:]:
        copy.wait()
    with jax.named_scope('proj'):
        for col in range(0, model, step):
            term = jnp.dot(attended, out_w[:, col : col + step], preferred_element_type=jnp.float32)
            projected[:, :, col : col + step] = term.astype(jnp.bfloat16).reshape(4, rows, step)

    def plus(one, two):
        return one.astype(jnp.float32) + two.astype(jnp.float32)

    pc_first = start(projected.at[diagonal], p_core.at[1], pc_send.at[1], pc_recv.at[1], to_core)
    pc_second = start(projected.at[core], p_core.at[0], pc_send.at[0], pc_recv.at[0], to_core)
    with jax.named_scope('pc1'):
        pc_first.wait_recv()
    projected[across] = plus(projected[across], p_core[1]).astype(jnp.bfloat16)
    px = start(projected.at[across], p_x, px_send, px_recv, to_x)

    swaps = [[], [], []]

    def forward(kind, shift):
        origin = lax.rem(here - shift + size, size)
        with jax.named_scope(f"cross{kind}_{shift}"):
            crossing[kind][shift - 1].wait_recv()
        held = piece(refs[kind][1], kind, origin, part)
        swaps[kind].append(
            start(held, held, y_send.at[kind, shift - 1], y_recv.at[kind, shift - 1], {"grp": 1 - part})
        )

    def settle(kind):
        for copy in locals_[kind]:
            copy.wait()
        for copy in swaps[kind]:
            copy.wait_recv()

    with jax.named_scope('pc2'):
        pc_second.wait_recv()
    total[...] = residual[...].astype(jnp.float32) + plus(projected[t], p_core[0])
    for item in ('01',):
        forward(0, int(item[1]))
    with jax.named_scope('px'):
        px.wait_recv()
    mixed = total[...] + p_x[...].astype(jnp.float32)
    total[...] = mixed
    tokens[here, t] = (
        mixed * lax.rsqrt(jnp.mean(mixed * mixed, axis=1, keepdims=True) + 1e-06) * gain[...]
    ).astype(jnp.bfloat16)

    own_block = tokens.at[here, t]

    def own_copy(way):
        target = here + 1 - 2 * way
        return remote(own_block, own_block, z_send.at[way], z_recv.at[here], {"sp": target})

    @pl.when(here < last)
    def _():
        own_copy(0).start()

    @pl.when(here > 0)
    def _():
        own_copy(1).start()

    def passing(i):
        origin = origins[i]
        block = tokens.at[origin, t]
        target = jnp.where(origin < here, here + 1, here - 1)
        valid = (target >= 0) & (target <= last)
        target = jnp.clip(target, 0, last)
        return valid, remote(block, block, z_send.at[1 + i], z_recv.at[origin], {"sp": target})

    x_copies, c_first, c_second, r_first, r_second, rx = {}, {}, {}, {}, {}, {}

    def step_a(i):
        o = origins[i]
        block = tokens.at[o, t]
        if i:
            with jax.named_scope(f'tokz{i}'):
                remote(block, block, z_send.at[1 + i], z_recv.at[o], to_x).wait_recv()
            valid, copy = passing(i)
            pl.when(valid)(copy.start)
        x_copies[i] = start(block, block, x_send.at[i], x_recv.at[i], to_x)
        c_first[i] = start(block, block, c_send.at[i, 0], c_recv.at[i, 0], to_core)

    def step_b(i):
        with jax.named_scope(f'tokx{i}'):
            x_copies[i].wait_recv()
        block = tokens.at[origins[i], across]
        c_second[i] = start(block, block, c_send.at[i, 1], c_recv.at[i, 1], to_core)

    tiles, per = column_tiles(hidden_columns)
    before = jnp.where(here > 0, window_start(jnp.maximum(here - 1, 0), hidden_columns) + per, 0)
    first = (before - window_start(here, hidden_columns)) * 128
    keep = lax.broadcasted_iota(jnp.int32, (1, width), 1) >= first

    def step_c(i):
        o = origins[i]
        c_first[i].wait_recv()
        with jax.named_scope(f'tokc{i}'):
            c_second[i].wait_recv()
        if i == 0:
            with jax.named_scope('settle01'):
                settle(0)
                settle(1)
        x = tokens[o].reshape(4 * rows, model)
        with jax.named_scope(f'gateup{i}'):
            gated = jnp.dot(x, gate_v[...], preferred_element_type=jnp.float32)
            lifted = jnp.dot(x, up_v[...], preferred_element_type=jnp.float32)
            fired = jnp.where(keep, gated / (1.0 + jnp.exp(-gated)) * lifted, 0.0).astype(jnp.bfloat16)
        hidden[o] = fired

    def step_f(j):
        origin = lax.rem(here - j + size, size)
        if j:
            with jax.named_scope(f"settle2_{j}"):
                swaps[2][j - 1].wait_recv()
        else:
            for copy in locals_[2]:
                copy.wait()
        fired = hidden[...].reshape(size * count, width)
        with jax.named_scope(f"downmm{j}"):
            held = pl.ds(pl.multiple_of(origin * outer, outer), outer)
            term = jnp.dot(fired, down_v[:, held], preferred_element_type=jnp.float32)
            parts[j] = term.astype(jnp.bfloat16).reshape(size, 4, rows, outer)
        r_first[j] = start(parts.at[j, :, diagonal], from_core.at[j, 1], rc_send.at[j, 1], rc_recv.at[j, 1], to_core)
        r_second[j] = start(parts.at[j, :, core], from_core.at[j, 0], rc_send.at[j, 0], rc_recv.at[j, 0], to_core)

    def step_d(j):
        with jax.named_scope(f"rc1_{j}"):
            r_first[j].wait_recv()
        parts[j, :, across] = plus(parts[j, :, across], from_core[j, 1]).astype(jnp.bfloat16)
        rx[j] = start(parts.at[j, :, across], from_x.at[j], rx_send.at[j], rx_recv.at[j], to_x)
        with jax.named_scope(f"rc2_{j}"):
            r_second[j].wait_recv()
        parts[j, :, t] = plus(parts[j, :, t], from_core[j, 0]).astype(jnp.bfloat16)

    def step_e(j):
        origin = lax.rem(here - j + size, size)
        with jax.named_scope(f"rx{j}"):
            rx[j].wait_recv()
        for i in range(size - 1, 0, -1):
            o = origins[i]
            parts[j, o, t] = plus(parts[j, o, t], from_x[j, o]).astype(jnp.bfloat16)
            start(parts.at[j, o, t], from_z.at[origin, here], rz_send.at[j, i], rz_recv.at[origin, here], {"sp": o})
        held = pl.ds(pl.multiple_of(origin * outer, outer), outer)
        total[:, held] = total[:, held] + plus(parts[j, here, t], from_x[j, here])

    steps = {
        "a": step_a, "b": step_b, "c": step_c, "d": step_d, "e": step_e, "f": step_f,
        "0": lambda shift: forward(0, shift), "1": lambda shift: forward(1, shift),
        "2": lambda shift: forward(2, shift), "s": spread,
    }
    for item in ('a0', '02', '03', '11', '12', '13', 'a1', 'b0', 'a2', 'c0', 'b1', 'a3', 's2', 'c1', 'b2', 'c2', 'b3', 'c3', 'f0', '21', 'd0', '22', 'f1', '23', 'd1', 'e0', 'f2', 'd2', 'e1', 'f3', 'd3', 'e2', 'e3'):
        steps[item[0]](int(item[1]))
    for place in range(size):
        held = slice(place * outer, (place + 1) * outer)
        result = total[:, held]
        for i in range(1, size):
            o = origins[i]
            with jax.named_scope(f"rz{place}_{i}"):
                remote(from_z.at[place, o], from_z.at[place, o], rz_send.at[0, i], rz_recv.at[place, o], to_x).wait_recv()
            result = result + from_z[place, o].astype(jnp.float32)
        out[:, held] = result.astype(out.dtype)

    @pl.when(here < last)
    def _():
        own_copy(0).wait_send()

    @pl.when(here > 0)
    def _():
        own_copy(1).wait_send()

    for i in range(1, size):
        valid, copy = passing(i)
        pl.when(valid)(copy.wait_send)
    for copy in pending:
        copy.wait_send()


def position_table(token_count, lanes):
    freqs = ROPE // 4
    lane = np.arange(lanes)
    place = np.arange(token_count)
    inverse = np.power(10000.0, -(lane % freqs).astype(np.float64) / freqs)
    grid = np.where((lane % ROPE < ROPE // 2)[None], (place // GRID_W)[:, None], (place % GRID_W)[:, None])
    angles = grid.astype(np.float64) * inverse[None]
    return np.stack([np.cos(angles), np.sin(angles)]).astype(np.float32)


def spread_layer(
    query_nope, query_rope, token_latent, key_rope, latent_norm_gain, key_w, value_w,
    residual, out_w, ffn_gain, gate_w, up_w, down_w,
):
    size = lax.axis_size("sp")
    depth, columns = gate_w.shape
    width = column_tiles(columns)[1] * 128
    count, model = residual.shape
    lanes = query_nope.shape[1]
    wide = token_latent.shape[1] + query_rope.shape[1]
    block = (count // 4, model)
    table = jnp.asarray(position_table(size * count, query_rope.shape[1]))
    dma = pltpu.SemaphoreType.DMA
    narrow = jnp.bfloat16
    vmem = lambda *lead: pltpu.VMEM(lead + block, narrow)
    slab = lambda *lead: pltpu.VMEM(lead + (block[0], down_w.shape[1]), narrow)
    square = [dma((size, size)), dma((size, size))]
    line = [dma((size - 1,)), dma((size - 1,))]
    line_pair = [dma((size - 1, 2)), dma((size - 1, 2))]
    pieces = [dma((3, size - 1)), dma((3, size - 1))]
    single = [dma((size,)), dma((size,))]
    double = [dma((size, 2)), dma((size, 2))]
    here = pl.BlockSpec(memory_space=pltpu.VMEM)
    away = pl.BlockSpec(memory_space=pl.ANY)
    return pl.pallas_call(
        functools.partial(layer_kernel, size, columns),
        out_shape=jax.ShapeDtypeStruct(block, narrow),
        in_specs=[here] * 5 + [away] * 5 + [here] + [away] * 3,
        out_specs=here,
        scratch_shapes=[
            pltpu.VMEM((key_w.shape[0], lanes), narrow),
            pltpu.VMEM((value_w.shape[0], lanes), narrow),
            pltpu.VMEM(out_w.shape, narrow),
            vmem(),
            pltpu.VMEM(table.shape, jnp.float32),
            pltpu.VMEM((size, count, wide), narrow),
            pltpu.VMEM((size * count, lanes + query_rope.shape[1]), narrow),
            pltpu.VMEM((size * count, lanes), narrow),
            pltpu.VMEM((size * depth, width), narrow),
            pltpu.VMEM((size * depth, width), narrow),
            pltpu.VMEM((width, size * down_w.shape[1]), narrow),
            vmem(4), vmem(2), vmem(),
            vmem(size, 4), slab(size, size, 4), pltpu.VMEM((size, count, width), narrow),
            slab(size, 2, size), slab(size, size), slab(size, size),
            pltpu.VMEM(block, jnp.float32),
            dma((5,)), dma((3, 2)), *pieces, *pieces,
            *line, *line, *line_pair,
            dma((2,)), dma((2,)), dma, dma,
            dma((size + 1,)), dma((size,)), *single, *double, *double, *single, *square,
        ],
        compiler_params=pltpu.CompilerParams(collective_id=0, has_side_effects=True),
        name="layer",
    )(
        query_nope, query_rope, token_latent, key_rope, latent_norm_gain[None],
        key_w, value_w, out_w, residual, table, ffn_gain[None], gate_w, up_w, down_w,
    )


def local(
    query_nope,
    query_rope,
    token_latent,
    key_rope,
    latent_norm_gain,
    key_expand_weight,
    value_expand_weight,
    residual,
    out_weight,
    ffn_gain,
    gate_weight,
    up_weight,
    down_weight,
):
    if spread_hidden(query_nope.shape[0] * lax.axis_size("sp"), gate_weight.shape[1]):
        return spread_layer(
            query_nope,
            query_rope,
            token_latent,
            key_rope,
            latent_norm_gain,
            key_expand_weight,
            value_expand_weight,
            residual,
            out_weight,
            ffn_gain,
            gate_weight,
            up_weight,
            down_weight,
        )
    tok_rows = query_nope.shape[0]
    heads_here = query_nope.shape[1] // UNROTATED_SIZE
    own_rows = tok_rows // lax.axis_size("tp")
    tp_index = lax.axis_index("tp")
    positions = lax.axis_index("sp") * tok_rows + jnp.arange(tok_rows, dtype=jnp.int32)
    query_flat = query_nope.reshape(tok_rows, heads_here, UNROTATED_SIZE)
    query_turned = turn_heads(
        query_rope.astype(jnp.float32).reshape(tok_rows, heads_here, ROPE), positions
    ).astype(jnp.bfloat16)
    latent = norm_rows(token_latent, latent_norm_gain).astype(jnp.bfloat16)
    key_turned = turn_heads(key_rope.astype(jnp.float32)[:, None, :], positions)[:, 0].astype(
        jnp.bfloat16
    )
    key_cols = lax.dynamic_slice_in_dim(
        key_expand_weight, tp_index * heads_here * UNROTATED_SIZE, heads_here * UNROTATED_SIZE, 1
    )
    value_cols = lax.dynamic_slice_in_dim(
        value_expand_weight, tp_index * heads_here * VALUE_SIZE, heads_here * VALUE_SIZE, 1
    )
    score_scale = (UNROTATED_SIZE + ROPE) ** (-0.5)

    def absorb(carried, block_in):
        latent_block, rope_block = block_in
        block_rows = latent_block.shape[0]
        key_rows = jnp.dot(latent_block, key_cols, preferred_element_type=jnp.float32).astype(
            jnp.bfloat16
        )
        key_rows = key_rows.reshape(block_rows, heads_here, UNROTATED_SIZE)
        value_rows = jnp.dot(latent_block, value_cols, preferred_element_type=jnp.float32).astype(
            jnp.bfloat16
        )
        value_rows = value_rows.reshape(block_rows, heads_here, VALUE_SIZE)
        scores = (
            jnp.einsum("qhd,khd->hqk", query_flat, key_rows, preferred_element_type=jnp.float32)
            + jnp.einsum(
                "qhd,kd->hqk", query_turned, rope_block, preferred_element_type=jnp.float32
            )
        ) * score_scale
        highest, totals, accumulated = carried
        new_highest = jnp.maximum(highest, jnp.max(scores, axis=-1))
        shrink = jnp.exp(highest - new_highest)
        weights = jnp.exp(scores - new_highest[:, :, None])
        totals = totals * shrink + jnp.sum(weights, axis=-1)
        accumulated = accumulated * shrink.T[:, :, None] + jnp.einsum(
            "hqk,khd->qhd",
            weights.astype(jnp.bfloat16),
            value_rows,
            preferred_element_type=jnp.float32,
        )
        return ((new_highest, totals, accumulated), None)

    initial = (
        jnp.full((heads_here, tok_rows), -jnp.inf, jnp.float32),
        jnp.zeros((heads_here, tok_rows), jnp.float32),
        jnp.zeros((tok_rows, heads_here, VALUE_SIZE), jnp.float32),
    )
    carried = initial
    latent_piece = lax.all_gather(latent, "sp", axis=0, tiled=True)
    rope_piece = lax.all_gather(key_turned, "sp", axis=0, tiled=True)
    shard_count = latent_piece.shape[0] // tok_rows
    grouped = max(
        (
            factor
            for factor in range(1, shard_count + 1)
            if shard_count % factor == 0 and factor * tok_rows <= max(1024, tok_rows)
        )
    )
    block_rows = grouped * tok_rows
    blocks = (
        latent_piece.reshape(-1, block_rows, latent_piece.shape[1]),
        rope_piece.reshape(-1, block_rows, rope_piece.shape[1]),
    )
    carried, _ = lax.scan(absorb, carried, blocks)
    highest, totals, accumulated = carried
    attended = (
        (accumulated / totals.T[:, :, None])
        .reshape(tok_rows, heads_here * VALUE_SIZE)
        .astype(jnp.bfloat16)
    )
    projected = jnp.dot(attended, out_weight, preferred_element_type=jnp.float32).astype(
        jnp.bfloat16
    )
    summed = lax.psum(projected, "tp").astype(jnp.float32)
    mixed_all = residual.astype(jnp.float32) + summed
    normed_all = norm_rows(mixed_all, ffn_gain).astype(jnp.bfloat16)
    mixed_own = lax.dynamic_slice_in_dim(mixed_all, tp_index * own_rows, own_rows, 0)
    gate_piece = lax.all_gather(gate_weight, "sp", axis=0, tiled=True)
    up_piece = lax.all_gather(up_weight, "sp", axis=0, tiled=True)
    gate = jnp.dot(normed_all, gate_piece, preferred_element_type=jnp.float32)
    up_part = jnp.dot(normed_all, up_piece, preferred_element_type=jnp.float32)
    hidden = (jax.nn.silu(gate) * up_part).astype(jnp.bfloat16)
    terms = jnp.dot(
        hidden,
        lax.all_gather(down_weight, "sp", axis=1, tiled=True),
        preferred_element_type=jnp.float32,
    )
    ffn_own = lax.psum_scatter(
        terms.astype(jnp.bfloat16), "tp", scatter_dimension=0, tiled=True
    ).astype(jnp.float32)
    return (mixed_own + ffn_own).astype(jnp.bfloat16)


def solution(mesh):
    return jax.shard_map(
        local,
        mesh=mesh,
        in_specs=(
            P(("grp", "sp"), "tp"),
            P(("grp", "sp"), "tp"),
            P(("grp", "sp"), None),
            P(("grp", "sp"), None),
            P(),
            P(),
            P(),
            P(("grp", "sp"), None),
            P("tp", None),
            P(),
            P("sp", "tp"),
            P("sp", "tp"),
            P("tp", "sp"),
        ),
        out_specs=P(("grp", "sp", "tp"), None),
        check_vma=False,
    )
```

```python
import functools

import jax
import jax.numpy as jnp
import numpy as np
from jax import lax
from jax.experimental import pallas as pl
from jax.experimental.pallas import tpu as pltpu
from jax.sharding import PartitionSpec as P

MESH = pl.DeviceIdType.MESH
UNROTATED_SIZE = 64
ROPE = 32
VALUE_SIZE = 64
GRID_W = 64


def norm_rows(values, gain):
    wide = values.astype(jnp.float32)
    return wide * lax.rsqrt(jnp.mean(wide * wide, axis=-1, keepdims=True) + 1e-06) * gain


def turn_heads(vectors, positions):
    tokens, heads, width = vectors.shape
    freqs = width // 4
    grid_pos = jnp.stack([positions // GRID_W, positions % GRID_W], axis=-1).astype(jnp.float32)
    inverse = jnp.power(10000.0, -jnp.arange(freqs, dtype=jnp.float32) / freqs)
    angles = grid_pos[:, :, None] * inverse
    cosine = jnp.cos(angles)[:, None]
    sine = jnp.sin(angles)[:, None]
    viewed = vectors.reshape(tokens, heads, 2, 2, freqs)
    first = viewed[..., 0, :]
    second = viewed[..., 1, :]
    turned = jnp.stack([first * cosine - second * sine, first * sine + second * cosine], axis=-2)
    return turned.reshape(tokens, heads, width)


def spread_hidden(token_count, hidden_columns):
    fits = lax.axis_size("tp") == 4 and lax.axis_size("grp") == 2
    return fits and 2 * token_count < 3 * hidden_columns


def column_tiles(hidden_columns):
    tiles = hidden_columns // 128
    return tiles, -(-tiles // lax.axis_size("sp"))


def window_start(at, parity, hidden_columns):
    tiles, per = column_tiles(hidden_columns)
    from_left = jnp.minimum(at * per, tiles - per)
    from_right = jnp.maximum(tiles - (lax.axis_size("sp") - at) * per, 0)
    return jnp.where(parity == 0, from_left, from_right)


class Either:
    def __init__(self, small_out, small_in, make):
        self.small_out, self.small_in, self.make = small_out, small_in, make

    def run(self, small, name):
        for value, chosen in ((False, jnp.logical_not(small)), (True, small)):

            @pl.when(chosen)
            def _():
                getattr(self.make(value), name)()

    def start(self):
        self.run(self.small_out, "start")

    def wait_send(self):
        self.run(self.small_out, "wait_send")

    def wait_recv(self):
        self.run(self.small_in, "wait_recv")

    def wait(self):
        self.run(self.small_out, "wait")


def signal_all(peers):
    barrier = pltpu.get_barrier_semaphore()
    for peer in peers:
        pl.semaphore_signal(barrier, inc=1, device_id=peer, device_id_type=MESH)
    pl.semaphore_wait(barrier, len(peers))


def remote(src, dst, send_sem, recv_sem, peer):
    return pltpu.make_async_remote_copy(
        src_ref=src,
        dst_ref=dst,
        send_sem=send_sem,
        recv_sem=recv_sem,
        device_id=peer,
        device_id_type=MESH,
    )


def line_order(here, size):
    table = []
    for at in range(size):
        others = [place for place in range(size) if place != at]
        flip = 1 if 2 * at < size else -1
        table.append(sorted(others, key=lambda place: (abs(place - at), (place - at) * flip)))
    columns = []
    for step in range(size - 1):
        value = jnp.int32(0)
        for at in range(size):
            value = value + jnp.where(here == at, table[at][step], 0)
        columns.append(value)
    return columns


def swap_matrix(lanes):
    freqs = ROPE // 4
    row = lax.broadcasted_iota(jnp.int32, (lanes, lanes), 0)
    lane = lax.broadcasted_iota(jnp.int32, (lanes, lanes), 1)
    first_half = lax.rem(lane, 2 * freqs) < freqs
    partner = jnp.where(first_half, lane + freqs, lane - freqs)
    sign = jnp.where(first_half, -1.0, 1.0)
    return jnp.where(row == partner, sign, 0.0).astype(jnp.bfloat16)


def layer_kernel(
    size, hidden_columns, query, query_rope, token_latent, key_rope, latent_gain,
    key_all, value_all, out_all, residual_all, table_all, gain, gate, up, down,
    out,
    key_w, value_w, out_w, residual, table, gathered, keys, values, gate_v, up_v, down_v, projected, p_core, p_x,
    tokens, parts, hidden, from_core, from_x, from_z, total,
    in_sem, own_sem, w_send, w_recv, y_send, y_recv,
    lz_send, lz_recv, lx_send, lx_recv, lc_send, lc_recv,
    pc_send, pc_recv, px_send, px_recv,
    z_send, z_recv, x_send, x_recv, c_send, c_recv,
    rc_send, rc_recv, rx_send, rx_recv, rz_send, rz_recv,
):
    here = lax.axis_index("sp")
    part = lax.axis_index("grp")
    t = lax.axis_index("tp")
    core = t + 1 - 2 * lax.rem(t, 2)
    across = t + 2 - 4 * lax.div(t, 2)
    diagonal = core + 2 - 4 * lax.div(core, 2)
    to_core, to_x = {"tp": core}, {"tp": across}
    depth = gate.shape[0]
    width = gate_v.shape[1]
    outer = down.shape[1]
    count = token_latent.shape[0]
    rank = token_latent.shape[1]
    rows = count // 4
    model = residual.shape[1]
    lanes = query.shape[1]
    columns = pl.ds(pl.multiple_of(t * lanes, 128), lanes)
    step = outer
    order = line_order(here, size)
    origins = [here] + order
    last = size - 1
    pending = []

    def start(*args):
        copy = remote(*args)
        copy.start()
        pending.append(copy)
        return copy

    parity = lax.rem(t, 2)
    tiles, per = column_tiles(hidden_columns)
    spare = (size * per - tiles) * 128
    inset = pl.multiple_of((1 - parity) * spare, 128)
    narrow = width - spare

    def small(at):
        return at == (1 - parity) * last

    def start_of(at):
        return pl.multiple_of(window_start(at, parity, hidden_columns) * 128, 128)

    def piece(ref, kind, origin, half, short):
        if kind < 2:
            step = depth // 2
            where = pl.ds(pl.multiple_of(origin * depth + half * step, step), step)
            return ref.at[where, pl.ds(inset, narrow) if short else pl.ds(0, width)]
        step = (narrow if short else width) // 2
        first = half * step + (inset if short else 0)
        return ref.at[
            pl.ds(pl.multiple_of(first, 64), step),
            pl.ds(pl.multiple_of(origin * outer, outer), outer),
        ]

    def source(ref, kind, target, half, short):
        first = start_of(target) + (inset if short else 0)
        if kind < 2:
            step = depth // 2
            return ref.at[
                pl.ds(pl.multiple_of(half * step, step), step),
                pl.ds(pl.multiple_of(first, 128), narrow if short else width),
            ]
        step = (narrow if short else width) // 2
        return ref.at[pl.ds(pl.multiple_of(first + half * step, 64), step), :]

    if spare:

        @pl.when(small(here))
        def _():
            unused = pl.ds(pl.multiple_of(parity * narrow, 128), spare)
            down_v[unused, :] = jnp.zeros((spare, size * outer), down_v.dtype)

    def quarter(at):
        return pl.ds(pl.multiple_of(at * rows, rows), rows)

    loads = [
        pltpu.make_async_copy(src, dst, in_sem.at[n])
        for n, (src, dst) in enumerate(
            (
                (table_all, table),
                (key_all.at[:, columns], key_w),
                (value_all.at[:, columns], value_w),
                (out_all, out_w),
                (residual_all.at[quarter(t), :], residual),
            )
        )
    ]
    for copy in loads:
        copy.start()
    rope_own = key_rope[...]
    repeats = query_rope.shape[1] // ROPE
    gathered[here, :, :rank] = token_latent[...]
    gathered[here, :, rank:] = jnp.concatenate([rope_own] * repeats, axis=1)

    peers = [{"sp": lax.rem(here + shift, size)} for shift in range(1, size)]
    with jax.named_scope('barrier'):
        signal_all(peers + [to_core, to_x, {"grp": 1 - part}])

    lz = []
    for shift in range(1, size):
        held = gathered.at[here, quarter(t), :]
        lz.append(
            start(held, held, lz_send.at[shift - 1], lz_recv.at[shift - 1], {"sp": lax.rem(here + shift, size)})
        )
    refs = ((gate, gate_v), (up, up_v), (down, down_v))
    crossing = [[], [], []]

    def weight_copy(kind, shift):
        ref, held = refs[kind]
        target = lax.rem(here + shift, size)
        return Either(
            small(target),
            small(here),
            lambda short: remote(
                source(ref, kind, target, part, short),
                piece(held, kind, here, part, short),
                w_send.at[kind, shift - 1],
                w_recv.at[kind, shift - 1],
                {"sp": target},
            ),
        )

    def own_weight(kind, half):
        ref, held = refs[kind]
        return Either(
            small(here),
            small(here),
            lambda short: pltpu.make_async_copy(
                source(ref, kind, here, half, short),
                piece(held, kind, here, half, short),
                own_sem.at[kind, half],
            ),
        )

    def swap_copy(kind, shift):
        origin = lax.rem(here - shift + size, size)

        def make(short):
            held = piece(refs[kind][1], kind, origin, part, short)
            return remote(
                held, held, y_send.at[kind, shift - 1], y_recv.at[kind, shift - 1], {"grp": 1 - part}
            )

        return Either(small(here), small(here), make)

    def spread(kind):
        for shift in range(1, size):
            crossing[kind].append(weight_copy(kind, shift))
            crossing[kind][-1].start()
        pending.extend(crossing[kind])

    locals_ = [[], [], []]
    for kind in range(3):
        for half in range(2):
            copy = own_weight(kind, half)
            copy.start()
            locals_[kind].append(copy)

    heads = lanes // UNROTATED_SIZE
    swap = swap_matrix(query_rope.shape[1])

    def turn(vectors, first):
        where = pl.ds(pl.multiple_of(first, 8), vectors.shape[0])
        other = jnp.dot(vectors, swap, preferred_element_type=jnp.float32)
        turned = vectors.astype(jnp.float32) * table[0, where, :] + other * table[1, where, :]
        return turned.astype(jnp.bfloat16)

    def expand(origin):
        where = pl.ds(pl.multiple_of(origin * count, count), count)
        latent = norm_rows(gathered[origin, :, :rank], latent_gain[...]).astype(jnp.bfloat16)
        keys[where, :lanes] = jnp.dot(
            latent, key_w[...], preferred_element_type=jnp.float32
        ).astype(jnp.bfloat16)
        keys[where, lanes:] = turn(gathered[origin, :, rank:], origin * count)
        values[where, :] = jnp.dot(
            latent, value_w[...], preferred_element_type=jnp.float32
        ).astype(jnp.bfloat16)

    for copy in loads[:3]:
        copy.wait()
    with jax.named_scope('own_kv'):
        turned = turn(query_rope[...], here * count)
        expand(here)
    lx, lc = {}, {}
    for shift in range(1, size):
        origin = lax.rem(here - shift + size, size)
        with jax.named_scope('lat_z'):
            lz[shift - 1].wait_recv()
        held = gathered.at[origin, quarter(t), :]
        lx[shift] = start(held, held, lx_send.at[shift - 1], lx_recv.at[shift - 1], to_x)
        lc[shift] = start(held, held, lc_send.at[shift - 1, 0], lc_recv.at[shift - 1, 0], to_core)
    spread(0)
    spread(1)
    lc_second = {}
    for shift in range(1, size):
        origin = lax.rem(here - shift + size, size)
        with jax.named_scope('lat_x'):
            lx[shift].wait_recv()
        held = gathered.at[origin, quarter(across), :]
        lc_second[shift] = start(held, held, lc_send.at[shift - 1, 1], lc_recv.at[shift - 1, 1], to_core)
    for shift in range(1, size):
        lc[shift].wait_recv()
        with jax.named_scope('lat_c'):
            lc_second[shift].wait_recv()
        with jax.named_scope('expand'):
            expand(lax.rem(here - shift + size, size))

    scale = (UNROTATED_SIZE + ROPE) ** (-0.5)
    lane = lax.broadcasted_iota(jnp.int32, (1, lanes), 1)
    rope_lane = lax.broadcasted_iota(jnp.int32, (1, turned.shape[1]), 1)
    attended = jnp.zeros((count, lanes), jnp.float32)
    with jax.named_scope('heads'):
        for head in range(heads):
            mine = (lane >= head * UNROTATED_SIZE) & (lane < (head + 1) * UNROTATED_SIZE)
            rope_mine = (rope_lane >= head * ROPE) & (rope_lane < (head + 1) * ROPE)
            both = jnp.concatenate(
                [
                    jnp.where(mine, query[...].astype(jnp.float32), 0.0),
                    jnp.where(rope_mine, turned.astype(jnp.float32), 0.0),
                ],
                axis=1,
            ).astype(jnp.bfloat16)
            scores = (
                lax.dot_general(
                    both, keys[...], (((1,), (1,)), ((), ())), preferred_element_type=jnp.float32
                )
                * scale
            )
            raised = jnp.exp(scores - jnp.max(scores, axis=1, keepdims=True))
            totals = jnp.sum(raised, axis=1, keepdims=True)
            weighted = jnp.dot(
                raised.astype(jnp.bfloat16), values[...], preferred_element_type=jnp.float32
            )
            attended = jnp.where(mine, weighted / totals, attended)
    attended = attended.astype(jnp.bfloat16)
    for copy in loads[3:]:
        copy.wait()
    with jax.named_scope('proj'):
        for col in range(0, model, step):
            term = jnp.dot(attended, out_w[:, col : col + step], preferred_element_type=jnp.float32)
            projected[:, :, col : col + step] = term.astype(jnp.bfloat16).reshape(4, rows, step)

    def plus(one, two):
        return one.astype(jnp.float32) + two.astype(jnp.float32)

    pc_first = start(projected.at[diagonal], p_core.at[1], pc_send.at[1], pc_recv.at[1], to_core)
    pc_second = start(projected.at[core], p_core.at[0], pc_send.at[0], pc_recv.at[0], to_core)
    with jax.named_scope('pc1'):
        pc_first.wait_recv()
    projected[across] = plus(projected[across], p_core[1]).astype(jnp.bfloat16)
    px = start(projected.at[across], p_x, px_send, px_recv, to_x)

    swaps = [[], [], []]

    def forward(kind, shift):
        with jax.named_scope(f"cross{kind}_{shift}"):
            crossing[kind][shift - 1].wait_recv()
        copy = swap_copy(kind, shift)
        copy.start()
        pending.append(copy)
        swaps[kind].append(copy)

    def settle(kind):
        for copy in locals_[kind]:
            copy.wait()
        for copy in swaps[kind]:
            copy.wait_recv()

    with jax.named_scope('pc2'):
        pc_second.wait_recv()
    total[...] = residual[...].astype(jnp.float32) + plus(projected[t], p_core[0])
    for item in ('01',):
        forward(0, int(item[1]))
    with jax.named_scope('px'):
        px.wait_recv()
    mixed = total[...] + p_x[...].astype(jnp.float32)
    total[...] = mixed
    tokens[here, t] = (
        mixed * lax.rsqrt(jnp.mean(mixed * mixed, axis=1, keepdims=True) + 1e-06) * gain[...]
    ).astype(jnp.bfloat16)

    own_block = tokens.at[here, t]

    def own_copy(way):
        target = here + 1 - 2 * way
        return remote(own_block, own_block, z_send.at[way], z_recv.at[here], {"sp": target})

    @pl.when(here < last)
    def _():
        own_copy(0).start()

    @pl.when(here > 0)
    def _():
        own_copy(1).start()

    def passing(i):
        origin = origins[i]
        block = tokens.at[origin, t]
        target = jnp.where(origin < here, here + 1, here - 1)
        valid = (target >= 0) & (target <= last)
        target = jnp.clip(target, 0, last)
        return valid, remote(block, block, z_send.at[1 + i], z_recv.at[origin], {"sp": target})

    x_copies, c_first, c_second, r_first, r_second, rx = {}, {}, {}, {}, {}, {}

    def step_a(i):
        o = origins[i]
        block = tokens.at[o, t]
        if i:
            with jax.named_scope(f'tokz{i}'):
                remote(block, block, z_send.at[1 + i], z_recv.at[o], to_x).wait_recv()
            valid, copy = passing(i)
            pl.when(valid)(copy.start)
        x_copies[i] = start(block, block, x_send.at[i], x_recv.at[i], to_x)
        c_first[i] = start(block, block, c_send.at[i, 0], c_recv.at[i, 0], to_core)

    def step_b(i):
        with jax.named_scope(f'tokx{i}'):
            x_copies[i].wait_recv()
        block = tokens.at[origins[i], across]
        c_second[i] = start(block, block, c_send.at[i, 1], c_recv.at[i, 1], to_core)

    column = lax.broadcasted_iota(jnp.int32, (1, width), 1)
    first_kept = jnp.where(small(here), inset, 0)
    kept = jnp.where(small(here), narrow, width)
    keep = (column >= first_kept) & (column < first_kept + kept)

    def step_c(i):
        o = origins[i]
        c_first[i].wait_recv()
        with jax.named_scope(f'tokc{i}'):
            c_second[i].wait_recv()
        if i == 0:
            with jax.named_scope('settle01'):
                settle(0)
                settle(1)
        x = tokens[o].reshape(4 * rows, model)
        with jax.named_scope(f'gateup{i}'):
            gated = jnp.dot(x, gate_v[...], preferred_element_type=jnp.float32)
            lifted = jnp.dot(x, up_v[...], preferred_element_type=jnp.float32)
            fired = jnp.where(keep, gated / (1.0 + jnp.exp(-gated)) * lifted, 0.0).astype(jnp.bfloat16)
        hidden[o] = fired

    def step_f(j):
        origin = lax.rem(here - j + size, size)
        if j:
            with jax.named_scope(f"settle2_{j}"):
                swaps[2][j - 1].wait_recv()
        else:
            for copy in locals_[2]:
                copy.wait()
        fired = hidden[...].reshape(size * count, width)
        with jax.named_scope(f"downmm{j}"):
            held = pl.ds(pl.multiple_of(origin * outer, outer), outer)
            term = jnp.dot(fired, down_v[:, held], preferred_element_type=jnp.float32)
            parts[j] = term.astype(jnp.bfloat16).reshape(size, 4, rows, outer)
        r_first[j] = start(parts.at[j, :, diagonal], from_core.at[j, 1], rc_send.at[j, 1], rc_recv.at[j, 1], to_core)
        r_second[j] = start(parts.at[j, :, core], from_core.at[j, 0], rc_send.at[j, 0], rc_recv.at[j, 0], to_core)

    def step_d(j):
        with jax.named_scope(f"rc1_{j}"):
            r_first[j].wait_recv()
        parts[j, :, across] = plus(parts[j, :, across], from_core[j, 1]).astype(jnp.bfloat16)
        rx[j] = start(parts.at[j, :, across], from_x.at[j], rx_send.at[j], rx_recv.at[j], to_x)
        with jax.named_scope(f"rc2_{j}"):
            r_second[j].wait_recv()
        parts[j, :, t] = plus(parts[j, :, t], from_core[j, 0]).astype(jnp.bfloat16)

    def step_e(j):
        origin = lax.rem(here - j + size, size)
        with jax.named_scope(f"rx{j}"):
            rx[j].wait_recv()
        for i in range(size - 1, 0, -1):
            o = origins[i]
            parts[j, o, t] = plus(parts[j, o, t], from_x[j, o]).astype(jnp.bfloat16)
            start(parts.at[j, o, t], from_z.at[origin, here], rz_send.at[j, i], rz_recv.at[origin, here], {"sp": o})
        held = pl.ds(pl.multiple_of(origin * outer, outer), outer)
        total[:, held] = total[:, held] + plus(parts[j, here, t], from_x[j, here])

    steps = {
        "a": step_a, "b": step_b, "c": step_c, "d": step_d, "e": step_e, "f": step_f,
        "0": lambda shift: forward(0, shift), "1": lambda shift: forward(1, shift),
        "2": lambda shift: forward(2, shift), "s": spread,
    }
    for item in ('a0', '02', '03', '11', '12', '13', 'a1', 'b0', 'a2', 'c0', 'b1', 'a3', 's2', 'c1', 'b2', 'c2', 'b3', 'c3', 'f0', '21', 'd0', '22', 'f1', '23', 'd1', 'e0', 'f2', 'd2', 'e1', 'f3', 'd3', 'e2', 'e3'):
        steps[item[0]](int(item[1]))
    for place in range(size):
        held = slice(place * outer, (place + 1) * outer)
        result = total[:, held]
        for i in range(1, size):
            o = origins[i]
            with jax.named_scope(f"rz{place}_{i}"):
                remote(from_z.at[place, o], from_z.at[place, o], rz_send.at[0, i], rz_recv.at[place, o], to_x).wait_recv()
            result = result + from_z[place, o].astype(jnp.float32)
        out[:, held] = result.astype(out.dtype)

    @pl.when(here < last)
    def _():
        own_copy(0).wait_send()

    @pl.when(here > 0)
    def _():
        own_copy(1).wait_send()

    for i in range(1, size):
        valid, copy = passing(i)
        pl.when(valid)(copy.wait_send)
    for copy in pending:
        copy.wait_send()


def position_table(token_count, lanes):
    freqs = ROPE // 4
    lane = np.arange(lanes)
    place = np.arange(token_count)
    inverse = np.power(10000.0, -(lane % freqs).astype(np.float64) / freqs)
    grid = np.where((lane % ROPE < ROPE // 2)[None], (place // GRID_W)[:, None], (place % GRID_W)[:, None])
    angles = grid.astype(np.float64) * inverse[None]
    return np.stack([np.cos(angles), np.sin(angles)]).astype(np.float32)


def spread_layer(
    query_nope, query_rope, token_latent, key_rope, latent_norm_gain, key_w, value_w,
    residual, out_w, ffn_gain, gate_w, up_w, down_w,
):
    size = lax.axis_size("sp")
    depth, columns = gate_w.shape
    width = column_tiles(columns)[1] * 128
    count, model = residual.shape
    lanes = query_nope.shape[1]
    wide = token_latent.shape[1] + query_rope.shape[1]
    block = (count // 4, model)
    table = jnp.asarray(position_table(size * count, query_rope.shape[1]))
    dma = pltpu.SemaphoreType.DMA
    narrow = jnp.bfloat16
    vmem = lambda *lead: pltpu.VMEM(lead + block, narrow)
    slab = lambda *lead: pltpu.VMEM(lead + (block[0], down_w.shape[1]), narrow)
    square = [dma((size, size)), dma((size, size))]
    line = [dma((size - 1,)), dma((size - 1,))]
    line_pair = [dma((size - 1, 2)), dma((size - 1, 2))]
    pieces = [dma((3, size - 1)), dma((3, size - 1))]
    single = [dma((size,)), dma((size,))]
    double = [dma((size, 2)), dma((size, 2))]
    here = pl.BlockSpec(memory_space=pltpu.VMEM)
    away = pl.BlockSpec(memory_space=pl.ANY)
    return pl.pallas_call(
        functools.partial(layer_kernel, size, columns),
        out_shape=jax.ShapeDtypeStruct(block, narrow),
        in_specs=[here] * 5 + [away] * 5 + [here] + [away] * 3,
        out_specs=here,
        scratch_shapes=[
            pltpu.VMEM((key_w.shape[0], lanes), narrow),
            pltpu.VMEM((value_w.shape[0], lanes), narrow),
            pltpu.VMEM(out_w.shape, narrow),
            vmem(),
            pltpu.VMEM(table.shape, jnp.float32),
            pltpu.VMEM((size, count, wide), narrow),
            pltpu.VMEM((size * count, lanes + query_rope.shape[1]), narrow),
            pltpu.VMEM((size * count, lanes), narrow),
            pltpu.VMEM((size * depth, width), narrow),
            pltpu.VMEM((size * depth, width), narrow),
            pltpu.VMEM((width, size * down_w.shape[1]), narrow),
            vmem(4), vmem(2), vmem(),
            vmem(size, 4), slab(size, size, 4), pltpu.VMEM((size, count, width), narrow),
            slab(size, 2, size), slab(size, size), slab(size, size),
            pltpu.VMEM(block, jnp.float32),
            dma((5,)), dma((3, 2)), *pieces, *pieces,
            *line, *line, *line_pair,
            dma((2,)), dma((2,)), dma, dma,
            dma((size + 1,)), dma((size,)), *single, *double, *double, *single, *square,
        ],
        compiler_params=pltpu.CompilerParams(collective_id=0, has_side_effects=True),
        name="layer",
    )(
        query_nope, query_rope, token_latent, key_rope, latent_norm_gain[None],
        key_w, value_w, out_w, residual, table, ffn_gain[None], gate_w, up_w, down_w,
    )


def local(
    query_nope,
    query_rope,
    token_latent,
    key_rope,
    latent_norm_gain,
    key_expand_weight,
    value_expand_weight,
    residual,
    out_weight,
    ffn_gain,
    gate_weight,
    up_weight,
    down_weight,
):
    if spread_hidden(query_nope.shape[0] * lax.axis_size("sp"), gate_weight.shape[1]):
        return spread_layer(
            query_nope,
            query_rope,
            token_latent,
            key_rope,
            latent_norm_gain,
            key_expand_weight,
            value_expand_weight,
            residual,
            out_weight,
            ffn_gain,
            gate_weight,
            up_weight,
            down_weight,
        )
    tok_rows = query_nope.shape[0]
    heads_here = query_nope.shape[1] // UNROTATED_SIZE
    own_rows = tok_rows // lax.axis_size("tp")
    tp_index = lax.axis_index("tp")
    positions = lax.axis_index("sp") * tok_rows + jnp.arange(tok_rows, dtype=jnp.int32)
    query_flat = query_nope.reshape(tok_rows, heads_here, UNROTATED_SIZE)
    query_turned = turn_heads(
        query_rope.astype(jnp.float32).reshape(tok_rows, heads_here, ROPE), positions
    ).astype(jnp.bfloat16)
    latent = norm_rows(token_latent, latent_norm_gain).astype(jnp.bfloat16)
    key_turned = turn_heads(key_rope.astype(jnp.float32)[:, None, :], positions)[:, 0].astype(
        jnp.bfloat16
    )
    key_cols = lax.dynamic_slice_in_dim(
        key_expand_weight, tp_index * heads_here * UNROTATED_SIZE, heads_here * UNROTATED_SIZE, 1
    )
    value_cols = lax.dynamic_slice_in_dim(
        value_expand_weight, tp_index * heads_here * VALUE_SIZE, heads_here * VALUE_SIZE, 1
    )
    score_scale = (UNROTATED_SIZE + ROPE) ** (-0.5)

    def absorb(carried, block_in):
        latent_block, rope_block = block_in
        block_rows = latent_block.shape[0]
        key_rows = jnp.dot(latent_block, key_cols, preferred_element_type=jnp.float32).astype(
            jnp.bfloat16
        )
        key_rows = key_rows.reshape(block_rows, heads_here, UNROTATED_SIZE)
        value_rows = jnp.dot(latent_block, value_cols, preferred_element_type=jnp.float32).astype(
            jnp.bfloat16
        )
        value_rows = value_rows.reshape(block_rows, heads_here, VALUE_SIZE)
        scores = (
            jnp.einsum("qhd,khd->hqk", query_flat, key_rows, preferred_element_type=jnp.float32)
            + jnp.einsum(
                "qhd,kd->hqk", query_turned, rope_block, preferred_element_type=jnp.float32
            )
        ) * score_scale
        highest, totals, accumulated = carried
        new_highest = jnp.maximum(highest, jnp.max(scores, axis=-1))
        shrink = jnp.exp(highest - new_highest)
        weights = jnp.exp(scores - new_highest[:, :, None])
        totals = totals * shrink + jnp.sum(weights, axis=-1)
        accumulated = accumulated * shrink.T[:, :, None] + jnp.einsum(
            "hqk,khd->qhd",
            weights.astype(jnp.bfloat16),
            value_rows,
            preferred_element_type=jnp.float32,
        )
        return ((new_highest, totals, accumulated), None)

    initial = (
        jnp.full((heads_here, tok_rows), -jnp.inf, jnp.float32),
        jnp.zeros((heads_here, tok_rows), jnp.float32),
        jnp.zeros((tok_rows, heads_here, VALUE_SIZE), jnp.float32),
    )
    carried = initial
    latent_piece = lax.all_gather(latent, "sp", axis=0, tiled=True)
    rope_piece = lax.all_gather(key_turned, "sp", axis=0, tiled=True)
    shard_count = latent_piece.shape[0] // tok_rows
    grouped = max(
        (
            factor
            for factor in range(1, shard_count + 1)
            if shard_count % factor == 0 and factor * tok_rows <= max(1024, tok_rows)
        )
    )
    block_rows = grouped * tok_rows
    blocks = (
        latent_piece.reshape(-1, block_rows, latent_piece.shape[1]),
        rope_piece.reshape(-1, block_rows, rope_piece.shape[1]),
    )
    carried, _ = lax.scan(absorb, carried, blocks)
    highest, totals, accumulated = carried
    attended = (
        (accumulated / totals.T[:, :, None])
        .reshape(tok_rows, heads_here * VALUE_SIZE)
        .astype(jnp.bfloat16)
    )
    projected = jnp.dot(attended, out_weight, preferred_element_type=jnp.float32).astype(
        jnp.bfloat16
    )
    summed = lax.psum(projected, "tp").astype(jnp.float32)
    mixed_all = residual.astype(jnp.float32) + summed
    normed_all = norm_rows(mixed_all, ffn_gain).astype(jnp.bfloat16)
    mixed_own = lax.dynamic_slice_in_dim(mixed_all, tp_index * own_rows, own_rows, 0)
    gate_piece = lax.all_gather(gate_weight, "sp", axis=0, tiled=True)
    up_piece = lax.all_gather(up_weight, "sp", axis=0, tiled=True)
    gate = jnp.dot(normed_all, gate_piece, preferred_element_type=jnp.float32)
    up_part = jnp.dot(normed_all, up_piece, preferred_element_type=jnp.float32)
    hidden = (jax.nn.silu(gate) * up_part).astype(jnp.bfloat16)
    terms = jnp.dot(
        hidden,
        lax.all_gather(down_weight, "sp", axis=1, tiled=True),
        preferred_element_type=jnp.float32,
    )
    ffn_own = lax.psum_scatter(
        terms.astype(jnp.bfloat16), "tp", scatter_dimension=0, tiled=True
    ).astype(jnp.float32)
    return (mixed_own + ffn_own).astype(jnp.bfloat16)


def solution(mesh):
    return jax.shard_map(
        local,
        mesh=mesh,
        in_specs=(
            P(("grp", "sp"), "tp"),
            P(("grp", "sp"), "tp"),
            P(("grp", "sp"), None),
            P(("grp", "sp"), None),
            P(),
            P(),
            P(),
            P(("grp", "sp"), None),
            P("tp", None),
            P(),
            P("sp", "tp"),
            P("sp", "tp"),
            P("tp", "sp"),
        ),
        out_specs=P(("grp", "sp", "tp"), None),
        check_vma=False,
    )
```

```python
import functools

import jax
import jax.numpy as jnp
import numpy as np
from jax import lax
from jax.experimental import pallas as pl
from jax.experimental.pallas import tpu as pltpu
from jax.sharding import PartitionSpec as P

MESH = pl.DeviceIdType.MESH
UNROTATED_SIZE = 64
ROPE = 32
VALUE_SIZE = 64
GRID_W = 64


def norm_rows(values, gain):
    wide = values.astype(jnp.float32)
    return wide * lax.rsqrt(jnp.mean(wide * wide, axis=-1, keepdims=True) + 1e-06) * gain


def turn_heads(vectors, positions):
    tokens, heads, width = vectors.shape
    freqs = width // 4
    grid_pos = jnp.stack([positions // GRID_W, positions % GRID_W], axis=-1).astype(jnp.float32)
    inverse = jnp.power(10000.0, -jnp.arange(freqs, dtype=jnp.float32) / freqs)
    angles = grid_pos[:, :, None] * inverse
    cosine = jnp.cos(angles)[:, None]
    sine = jnp.sin(angles)[:, None]
    viewed = vectors.reshape(tokens, heads, 2, 2, freqs)
    first = viewed[..., 0, :]
    second = viewed[..., 1, :]
    turned = jnp.stack([first * cosine - second * sine, first * sine + second * cosine], axis=-2)
    return turned.reshape(tokens, heads, width)


def spread_hidden(token_count, hidden_columns):
    fits = lax.axis_size("tp") == 4 and lax.axis_size("grp") == 2
    return fits and 2 * token_count < 3 * hidden_columns


def column_tiles(hidden_columns):
    tiles = hidden_columns // 128
    return tiles, -(-tiles // lax.axis_size("sp"))


def window_start(at, parity, hidden_columns):
    tiles, per = column_tiles(hidden_columns)
    from_left = jnp.minimum(at * per, tiles - per)
    from_right = jnp.maximum(tiles - (lax.axis_size("sp") - at) * per, 0)
    return jnp.where(parity == 0, from_left, from_right)


class Either:
    def __init__(self, small_out, small_in, make):
        self.small_out, self.small_in, self.make = small_out, small_in, make

    def run(self, small, name):
        for value, chosen in ((False, jnp.logical_not(small)), (True, small)):

            @pl.when(chosen)
            def _():
                getattr(self.make(value), name)()

    def start(self):
        self.run(self.small_out, "start")

    def wait_send(self):
        self.run(self.small_out, "wait_send")

    def wait_recv(self):
        self.run(self.small_in, "wait_recv")

    def wait(self):
        self.run(self.small_out, "wait")


def signal_all(peers):
    barrier = pltpu.get_barrier_semaphore()
    for peer in peers:
        pl.semaphore_signal(barrier, inc=1, device_id=peer, device_id_type=MESH)
    pl.semaphore_wait(barrier, len(peers))


def remote(src, dst, send_sem, recv_sem, peer):
    return pltpu.make_async_remote_copy(
        src_ref=src,
        dst_ref=dst,
        send_sem=send_sem,
        recv_sem=recv_sem,
        device_id=peer,
        device_id_type=MESH,
    )


def line_order(here, size):
    table = []
    for at in range(size):
        others = [place for place in range(size) if place != at]
        flip = 1 if 2 * at < size else -1
        table.append(sorted(others, key=lambda place: (abs(place - at), (place - at) * flip)))
    columns = []
    for step in range(size - 1):
        value = jnp.int32(0)
        for at in range(size):
            value = value + jnp.where(here == at, table[at][step], 0)
        columns.append(value)
    return columns


def swap_matrix(lanes):
    freqs = ROPE // 4
    row = lax.broadcasted_iota(jnp.int32, (lanes, lanes), 0)
    lane = lax.broadcasted_iota(jnp.int32, (lanes, lanes), 1)
    first_half = lax.rem(lane, 2 * freqs) < freqs
    partner = jnp.where(first_half, lane + freqs, lane - freqs)
    sign = jnp.where(first_half, -1.0, 1.0)
    return jnp.where(row == partner, sign, 0.0).astype(jnp.bfloat16)


def layer_kernel(
    size, hidden_columns, query, query_rope, token_latent, key_rope, latent_gain,
    key_all, value_all, out_all, residual_all, table_all, gain, gate, up, down,
    out,
    key_w, value_w, out_w, residual, table, gathered, keys, values, gate_v, up_v, down_v, projected, p_core, p_x,
    tokens, parts, hidden, from_core, from_x, from_z, total,
    in_sem, own_sem, w_send, w_recv, y_send, y_recv,
    lz_send, lz_recv, lx_send, lx_recv, lc_send, lc_recv,
    pc_send, pc_recv, px_send, px_recv,
    z_send, z_recv, x_send, x_recv, c_send, c_recv,
    rc_send, rc_recv, rx_send, rx_recv, rz_send, rz_recv,
):
    here = lax.axis_index("sp")
    part = lax.axis_index("grp")
    t = lax.axis_index("tp")
    core = t + 1 - 2 * lax.rem(t, 2)
    across = t + 2 - 4 * lax.div(t, 2)
    diagonal = core + 2 - 4 * lax.div(core, 2)
    to_core, to_x = {"tp": core}, {"tp": across}
    depth = gate.shape[0]
    width = gate_v.shape[1]
    outer = down.shape[1]
    count = token_latent.shape[0]
    rank = token_latent.shape[1]
    rows = count // 4
    model = residual.shape[1]
    lanes = query.shape[1]
    columns = pl.ds(pl.multiple_of(t * lanes, 128), lanes)
    step = outer
    order = line_order(here, size)
    origins = [here] + order
    last = size - 1
    pending = []

    def start(*args):
        copy = remote(*args)
        copy.start()
        pending.append(copy)
        return copy

    parity = lax.rem(t, 2)
    tiles, per = column_tiles(hidden_columns)
    spare = (size * per - tiles) * 128
    inset = pl.multiple_of((1 - parity) * spare, 128)
    narrow = width - spare

    def small(at):
        return at == (1 - parity) * last

    def start_of(at):
        return pl.multiple_of(window_start(at, parity, hidden_columns) * 128, 128)

    def piece(ref, kind, origin, half, short):
        if kind < 2:
            step = depth // 2
            where = pl.ds(pl.multiple_of(origin * depth + half * step, step), step)
            return ref.at[where, pl.ds(inset, narrow) if short else pl.ds(0, width)]
        step = (narrow if short else width) // 2
        first = half * step + (inset if short else 0)
        return ref.at[
            pl.ds(pl.multiple_of(first, 64), step),
            pl.ds(pl.multiple_of(origin * outer, outer), outer),
        ]

    def source(ref, kind, target, half, short):
        first = start_of(target) + (inset if short else 0)
        if kind < 2:
            step = depth // 2
            return ref.at[
                pl.ds(pl.multiple_of(half * step, step), step),
                pl.ds(pl.multiple_of(first, 128), narrow if short else width),
            ]
        step = (narrow if short else width) // 2
        return ref.at[pl.ds(pl.multiple_of(first + half * step, 64), step), :]

    if spare:

        @pl.when(small(here))
        def _():
            unused = pl.ds(pl.multiple_of(parity * narrow, 128), spare)
            down_v[unused, :] = jnp.zeros((spare, size * outer), down_v.dtype)

    def quarter(at):
        return pl.ds(pl.multiple_of(at * rows, rows), rows)

    loads = [
        pltpu.make_async_copy(src, dst, in_sem.at[n])
        for n, (src, dst) in enumerate(
            (
                (table_all, table),
                (key_all.at[:, columns], key_w),
                (value_all.at[:, columns], value_w),
                (out_all, out_w),
                (residual_all.at[quarter(t), :], residual),
            )
        )
    ]
    for copy in loads:
        copy.start()
    rope_own = key_rope[...]
    repeats = query_rope.shape[1] // ROPE
    gathered[here, :, :rank] = token_latent[...]
    gathered[here, :, rank:] = jnp.concatenate([rope_own] * repeats, axis=1)

    peers = [{"sp": lax.rem(here + shift, size)} for shift in range(1, size)]
    with jax.named_scope('barrier'):
        signal_all(peers + [to_core, to_x, {"grp": 1 - part}])

    lz = []
    for shift in range(1, size):
        held = gathered.at[here, quarter(t), :]
        lz.append(
            start(held, held, lz_send.at[shift - 1], lz_recv.at[shift - 1], {"sp": lax.rem(here + shift, size)})
        )
    refs = ((gate, gate_v), (up, up_v), (down, down_v))
    crossing = [[], [], []]

    def weight_copy(kind, shift):
        ref, held = refs[kind]
        target = lax.rem(here + shift, size)
        return Either(
            small(target),
            small(here),
            lambda short: remote(
                source(ref, kind, target, part, short),
                piece(held, kind, here, part, short),
                w_send.at[kind, shift - 1],
                w_recv.at[kind, shift - 1],
                {"sp": target},
            ),
        )

    def own_weight(kind, half):
        ref, held = refs[kind]
        return Either(
            small(here),
            small(here),
            lambda short: pltpu.make_async_copy(
                source(ref, kind, here, half, short),
                piece(held, kind, here, half, short),
                own_sem.at[kind, half],
            ),
        )

    def swap_copy(kind, shift):
        origin = lax.rem(here - shift + size, size)

        def make(short):
            held = piece(refs[kind][1], kind, origin, part, short)
            return remote(
                held, held, y_send.at[kind, shift - 1], y_recv.at[kind, shift - 1], {"grp": 1 - part}
            )

        return Either(small(here), small(here), make)

    def spread(kind):
        for shift in range(1, size):
            crossing[kind].append(weight_copy(kind, shift))
            crossing[kind][-1].start()
        pending.extend(crossing[kind])

    locals_ = [[], [], []]
    for kind in range(3):
        for half in range(2):
            copy = own_weight(kind, half)
            copy.start()
            locals_[kind].append(copy)

    heads = lanes // UNROTATED_SIZE
    swap = swap_matrix(query_rope.shape[1])

    def turn(vectors, first):
        where = pl.ds(pl.multiple_of(first, 8), vectors.shape[0])
        other = jnp.dot(vectors, swap, preferred_element_type=jnp.float32)
        turned = vectors.astype(jnp.float32) * table[0, where, :] + other * table[1, where, :]
        return turned.astype(jnp.bfloat16)

    def expand(origin):
        where = pl.ds(pl.multiple_of(origin * count, count), count)
        latent = norm_rows(gathered[origin, :, :rank], latent_gain[...]).astype(jnp.bfloat16)
        keys[where, :lanes] = jnp.dot(
            latent, key_w[...], preferred_element_type=jnp.float32
        ).astype(jnp.bfloat16)
        keys[where, lanes:] = turn(gathered[origin, :, rank:], origin * count)
        values[where, :] = jnp.dot(
            latent, value_w[...], preferred_element_type=jnp.float32
        ).astype(jnp.bfloat16)

    for copy in loads[:3]:
        copy.wait()
    with jax.named_scope('own_kv'):
        turned = turn(query_rope[...], here * count)
        expand(here)
    lx, lc = {}, {}
    for shift in range(1, size):
        origin = lax.rem(here - shift + size, size)
        with jax.named_scope('lat_z'):
            lz[shift - 1].wait_recv()
        held = gathered.at[origin, quarter(t), :]
        lx[shift] = start(held, held, lx_send.at[shift - 1], lx_recv.at[shift - 1], to_x)
        lc[shift] = start(held, held, lc_send.at[shift - 1, 0], lc_recv.at[shift - 1, 0], to_core)
    spread(0)
    spread(1)
    lc_second = {}
    for shift in range(1, size):
        origin = lax.rem(here - shift + size, size)
        with jax.named_scope('lat_x'):
            lx[shift].wait_recv()
        held = gathered.at[origin, quarter(across), :]
        lc_second[shift] = start(held, held, lc_send.at[shift - 1, 1], lc_recv.at[shift - 1, 1], to_core)
    for shift in range(1, size):
        lc[shift].wait_recv()
        with jax.named_scope('lat_c'):
            lc_second[shift].wait_recv()
        with jax.named_scope('expand'):
            expand(lax.rem(here - shift + size, size))

    scale = (UNROTATED_SIZE + ROPE) ** (-0.5)
    lane = lax.broadcasted_iota(jnp.int32, (1, lanes), 1)
    rope_lane = lax.broadcasted_iota(jnp.int32, (1, turned.shape[1]), 1)
    attended = jnp.zeros((count, lanes), jnp.float32)
    with jax.named_scope('heads'):
        for head in range(heads):
            mine = (lane >= head * UNROTATED_SIZE) & (lane < (head + 1) * UNROTATED_SIZE)
            rope_mine = (rope_lane >= head * ROPE) & (rope_lane < (head + 1) * ROPE)
            both = jnp.concatenate(
                [
                    jnp.where(mine, query[...].astype(jnp.float32), 0.0),
                    jnp.where(rope_mine, turned.astype(jnp.float32), 0.0),
                ],
                axis=1,
            ).astype(jnp.bfloat16)
            scores = (
                lax.dot_general(
                    both, keys[...], (((1,), (1,)), ((), ())), preferred_element_type=jnp.float32
                )
                * scale
            )
            raised = jnp.exp(scores - jnp.max(scores, axis=1, keepdims=True))
            totals = jnp.sum(raised, axis=1, keepdims=True)
            weighted = jnp.dot(
                raised.astype(jnp.bfloat16), values[...], preferred_element_type=jnp.float32
            )
            attended = jnp.where(mine, weighted / totals, attended)
    attended = attended.astype(jnp.bfloat16)
    for copy in loads[3:]:
        copy.wait()
    with jax.named_scope('proj'):
        for col in range(0, model, step):
            term = jnp.dot(attended, out_w[:, col : col + step], preferred_element_type=jnp.float32)
            projected[:, :, col : col + step] = term.astype(jnp.bfloat16).reshape(4, rows, step)

    def plus(one, two):
        return one.astype(jnp.float32) + two.astype(jnp.float32)

    pc_first = start(projected.at[diagonal], p_core.at[1], pc_send.at[1], pc_recv.at[1], to_core)
    pc_second = start(projected.at[core], p_core.at[0], pc_send.at[0], pc_recv.at[0], to_core)
    with jax.named_scope('pc1'):
        pc_first.wait_recv()
    projected[across] = plus(projected[across], p_core[1]).astype(jnp.bfloat16)
    px = start(projected.at[across], p_x, px_send, px_recv, to_x)

    swaps = [[], [], []]

    def forward(kind, shift):
        with jax.named_scope(f"cross{kind}_{shift}"):
            crossing[kind][shift - 1].wait_recv()
        copy = swap_copy(kind, shift)
        copy.start()
        pending.append(copy)
        swaps[kind].append(copy)

    def settle(kind):
        for copy in locals_[kind]:
            copy.wait()
        for copy in swaps[kind]:
            copy.wait_recv()

    with jax.named_scope('pc2'):
        pc_second.wait_recv()
    total[...] = residual[...].astype(jnp.float32) + plus(projected[t], p_core[0])
    for item in ('01',):
        forward(0, int(item[1]))
    with jax.named_scope('px'):
        px.wait_recv()
    mixed = total[...] + p_x[...].astype(jnp.float32)
    total[...] = mixed
    tokens[here, t] = (
        mixed * lax.rsqrt(jnp.mean(mixed * mixed, axis=1, keepdims=True) + 1e-06) * gain[...]
    ).astype(jnp.bfloat16)

    own_block = tokens.at[here, t]

    def own_copy(way):
        target = here + 1 - 2 * way
        return remote(own_block, own_block, z_send.at[way], z_recv.at[here], {"sp": target})

    @pl.when(here < last)
    def _():
        own_copy(0).start()

    @pl.when(here > 0)
    def _():
        own_copy(1).start()

    def passing(i):
        origin = origins[i]
        block = tokens.at[origin, t]
        target = jnp.where(origin < here, here + 1, here - 1)
        valid = (target >= 0) & (target <= last)
        target = jnp.clip(target, 0, last)
        return valid, remote(block, block, z_send.at[1 + i], z_recv.at[origin], {"sp": target})

    x_copies, c_first, c_second, r_first, r_second, rx = {}, {}, {}, {}, {}, {}

    def step_a(i):
        o = origins[i]
        block = tokens.at[o, t]
        if i:
            with jax.named_scope(f'tokz{i}'):
                remote(block, block, z_send.at[1 + i], z_recv.at[o], to_x).wait_recv()
            valid, copy = passing(i)
            pl.when(valid)(copy.start)
        x_copies[i] = start(block, block, x_send.at[i], x_recv.at[i], to_x)
        c_first[i] = start(block, block, c_send.at[i, 0], c_recv.at[i, 0], to_core)

    def step_b(i):
        with jax.named_scope(f'tokx{i}'):
            x_copies[i].wait_recv()
        block = tokens.at[origins[i], across]
        c_second[i] = start(block, block, c_send.at[i, 1], c_recv.at[i, 1], to_core)

    column = lax.broadcasted_iota(jnp.int32, (1, width), 1)
    first_kept = jnp.where(small(here), inset, 0)
    kept = jnp.where(small(here), narrow, width)
    keep = (column >= first_kept) & (column < first_kept + kept)

    def step_c(i):
        o = origins[i]
        c_first[i].wait_recv()
        with jax.named_scope(f'tokc{i}'):
            c_second[i].wait_recv()
        if i == 0:
            with jax.named_scope('settle01'):
                settle(0)
                settle(1)
        x = tokens[o].reshape(4 * rows, model)
        with jax.named_scope(f'gateup{i}'):
            gated = jnp.dot(x, gate_v[...], preferred_element_type=jnp.float32)
            lifted = jnp.dot(x, up_v[...], preferred_element_type=jnp.float32)
            fired = jnp.where(keep, gated / (1.0 + jnp.exp(-gated)) * lifted, 0.0).astype(jnp.bfloat16)
        hidden[o] = fired

    def step_f(j):
        origin = lax.rem(here - j + size, size)
        if j:
            with jax.named_scope(f"settle2_{j}"):
                swaps[2][j - 1].wait_recv()
        else:
            for copy in locals_[2]:
                copy.wait()
        fired = hidden[...].reshape(size * count, width)
        with jax.named_scope(f"downmm{j}"):
            held = pl.ds(pl.multiple_of(origin * outer, outer), outer)
            term = jnp.dot(fired, down_v[:, held], preferred_element_type=jnp.float32)
            parts[j] = term.astype(jnp.bfloat16).reshape(size, 4, rows, outer)
        r_first[j] = start(parts.at[j, :, diagonal], from_core.at[j, 1], rc_send.at[j, 1], rc_recv.at[j, 1], to_core)
        r_second[j] = start(parts.at[j, :, core], from_core.at[j, 0], rc_send.at[j, 0], rc_recv.at[j, 0], to_core)

    def step_d(j):
        with jax.named_scope(f"rc1_{j}"):
            r_first[j].wait_recv()
        parts[j, :, across] = plus(parts[j, :, across], from_core[j, 1]).astype(jnp.bfloat16)
        for i in range(size - 1, -1, -1):
            o = origins[i]
            rx[j, i] = start(
                parts.at[j, o, across], from_x.at[j, o], rx_send.at[j, i], rx_recv.at[j, i], to_x
            )
        with jax.named_scope(f"rc2_{j}"):
            r_second[j].wait_recv()
        parts[j, :, t] = plus(parts[j, :, t], from_core[j, 0]).astype(jnp.bfloat16)

    def step_e(j):
        origin = lax.rem(here - j + size, size)
        for i in range(size - 1, 0, -1):
            o = origins[i]
            with jax.named_scope(f"rx{j}"):
                rx[j, i].wait_recv()
            parts[j, o, t] = plus(parts[j, o, t], from_x[j, o]).astype(jnp.bfloat16)
            start(parts.at[j, o, t], from_z.at[origin, here], rz_send.at[j, i], rz_recv.at[origin, here], {"sp": o})
        rx[j, 0].wait_recv()
        held = pl.ds(pl.multiple_of(origin * outer, outer), outer)
        total[:, held] = total[:, held] + plus(parts[j, here, t], from_x[j, here])

    steps = {
        "a": step_a, "b": step_b, "c": step_c, "d": step_d, "e": step_e, "f": step_f,
        "0": lambda shift: forward(0, shift), "1": lambda shift: forward(1, shift),
        "2": lambda shift: forward(2, shift), "s": spread,
    }
    for item in ('a0', '02', '03', '11', '12', '13', 'a1', 'b0', 'a2', 'c0', 'b1', 'a3', 's2', 'c1', 'b2', 'c2', 'b3', 'c3', 'f0', '21', 'd0', '22', 'f1', '23', 'd1', 'e0', 'f2', 'd2', 'e1', 'f3', 'd3', 'e2', 'e3'):
        steps[item[0]](int(item[1]))
    for place in range(size):
        held = slice(place * outer, (place + 1) * outer)
        result = total[:, held]
        for i in range(1, size):
            o = origins[i]
            with jax.named_scope(f"rz{place}_{i}"):
                remote(from_z.at[place, o], from_z.at[place, o], rz_send.at[0, i], rz_recv.at[place, o], to_x).wait_recv()
            result = result + from_z[place, o].astype(jnp.float32)
        out[:, held] = result.astype(out.dtype)

    @pl.when(here < last)
    def _():
        own_copy(0).wait_send()

    @pl.when(here > 0)
    def _():
        own_copy(1).wait_send()

    for i in range(1, size):
        valid, copy = passing(i)
        pl.when(valid)(copy.wait_send)
    for copy in pending:
        copy.wait_send()


def position_table(token_count, lanes):
    freqs = ROPE // 4
    lane = np.arange(lanes)
    place = np.arange(token_count)
    inverse = np.power(10000.0, -(lane % freqs).astype(np.float64) / freqs)
    grid = np.where((lane % ROPE < ROPE // 2)[None], (place // GRID_W)[:, None], (place % GRID_W)[:, None])
    angles = grid.astype(np.float64) * inverse[None]
    return np.stack([np.cos(angles), np.sin(angles)]).astype(np.float32)


def spread_layer(
    query_nope, query_rope, token_latent, key_rope, latent_norm_gain, key_w, value_w,
    residual, out_w, ffn_gain, gate_w, up_w, down_w,
):
    size = lax.axis_size("sp")
    depth, columns = gate_w.shape
    width = column_tiles(columns)[1] * 128
    count, model = residual.shape
    lanes = query_nope.shape[1]
    wide = token_latent.shape[1] + query_rope.shape[1]
    block = (count // 4, model)
    table = jnp.asarray(position_table(size * count, query_rope.shape[1]))
    dma = pltpu.SemaphoreType.DMA
    narrow = jnp.bfloat16
    vmem = lambda *lead: pltpu.VMEM(lead + block, narrow)
    slab = lambda *lead: pltpu.VMEM(lead + (block[0], down_w.shape[1]), narrow)
    square = [dma((size, size)), dma((size, size))]
    line = [dma((size - 1,)), dma((size - 1,))]
    line_pair = [dma((size - 1, 2)), dma((size - 1, 2))]
    pieces = [dma((3, size - 1)), dma((3, size - 1))]
    single = [dma((size,)), dma((size,))]
    double = [dma((size, 2)), dma((size, 2))]
    here = pl.BlockSpec(memory_space=pltpu.VMEM)
    away = pl.BlockSpec(memory_space=pl.ANY)
    return pl.pallas_call(
        functools.partial(layer_kernel, size, columns),
        out_shape=jax.ShapeDtypeStruct(block, narrow),
        in_specs=[here] * 5 + [away] * 5 + [here] + [away] * 3,
        out_specs=here,
        scratch_shapes=[
            pltpu.VMEM((key_w.shape[0], lanes), narrow),
            pltpu.VMEM((value_w.shape[0], lanes), narrow),
            pltpu.VMEM(out_w.shape, narrow),
            vmem(),
            pltpu.VMEM(table.shape, jnp.float32),
            pltpu.VMEM((size, count, wide), narrow),
            pltpu.VMEM((size * count, lanes + query_rope.shape[1]), narrow),
            pltpu.VMEM((size * count, lanes), narrow),
            pltpu.VMEM((size * depth, width), narrow),
            pltpu.VMEM((size * depth, width), narrow),
            pltpu.VMEM((width, size * down_w.shape[1]), narrow),
            vmem(4), vmem(2), vmem(),
            vmem(size, 4), slab(size, size, 4), pltpu.VMEM((size, count, width), narrow),
            slab(size, 2, size), slab(size, size), slab(size, size),
            pltpu.VMEM(block, jnp.float32),
            dma((5,)), dma((3, 2)), *pieces, *pieces,
            *line, *line, *line_pair,
            dma((2,)), dma((2,)), dma, dma,
            dma((size + 1,)), dma((size,)), *single, *double, *double, *square, *square,
        ],
        compiler_params=pltpu.CompilerParams(collective_id=0, has_side_effects=True),
        name="layer",
    )(
        query_nope, query_rope, token_latent, key_rope, latent_norm_gain[None],
        key_w, value_w, out_w, residual, table, ffn_gain[None], gate_w, up_w, down_w,
    )


def local(
    query_nope,
    query_rope,
    token_latent,
    key_rope,
    latent_norm_gain,
    key_expand_weight,
    value_expand_weight,
    residual,
    out_weight,
    ffn_gain,
    gate_weight,
    up_weight,
    down_weight,
):
    if spread_hidden(query_nope.shape[0] * lax.axis_size("sp"), gate_weight.shape[1]):
        return spread_layer(
            query_nope,
            query_rope,
            token_latent,
            key_rope,
            latent_norm_gain,
            key_expand_weight,
            value_expand_weight,
            residual,
            out_weight,
            ffn_gain,
            gate_weight,
            up_weight,
            down_weight,
        )
    tok_rows = query_nope.shape[0]
    heads_here = query_nope.shape[1] // UNROTATED_SIZE
    own_rows = tok_rows // lax.axis_size("tp")
    tp_index = lax.axis_index("tp")
    positions = lax.axis_index("sp") * tok_rows + jnp.arange(tok_rows, dtype=jnp.int32)
    query_flat = query_nope.reshape(tok_rows, heads_here, UNROTATED_SIZE)
    query_turned = turn_heads(
        query_rope.astype(jnp.float32).reshape(tok_rows, heads_here, ROPE), positions
    ).astype(jnp.bfloat16)
    latent = norm_rows(token_latent, latent_norm_gain).astype(jnp.bfloat16)
    key_turned = turn_heads(key_rope.astype(jnp.float32)[:, None, :], positions)[:, 0].astype(
        jnp.bfloat16
    )
    key_cols = lax.dynamic_slice_in_dim(
        key_expand_weight, tp_index * heads_here * UNROTATED_SIZE, heads_here * UNROTATED_SIZE, 1
    )
    value_cols = lax.dynamic_slice_in_dim(
        value_expand_weight, tp_index * heads_here * VALUE_SIZE, heads_here * VALUE_SIZE, 1
    )
    score_scale = (UNROTATED_SIZE + ROPE) ** (-0.5)

    def absorb(carried, block_in):
        latent_block, rope_block = block_in
        block_rows = latent_block.shape[0]
        key_rows = jnp.dot(latent_block, key_cols, preferred_element_type=jnp.float32).astype(
            jnp.bfloat16
        )
        key_rows = key_rows.reshape(block_rows, heads_here, UNROTATED_SIZE)
        value_rows = jnp.dot(latent_block, value_cols, preferred_element_type=jnp.float32).astype(
            jnp.bfloat16
        )
        value_rows = value_rows.reshape(block_rows, heads_here, VALUE_SIZE)
        scores = (
            jnp.einsum("qhd,khd->hqk", query_flat, key_rows, preferred_element_type=jnp.float32)
            + jnp.einsum(
                "qhd,kd->hqk", query_turned, rope_block, preferred_element_type=jnp.float32
            )
        ) * score_scale
        highest, totals, accumulated = carried
        new_highest = jnp.maximum(highest, jnp.max(scores, axis=-1))
        shrink = jnp.exp(highest - new_highest)
        weights = jnp.exp(scores - new_highest[:, :, None])
        totals = totals * shrink + jnp.sum(weights, axis=-1)
        accumulated = accumulated * shrink.T[:, :, None] + jnp.einsum(
            "hqk,khd->qhd",
            weights.astype(jnp.bfloat16),
            value_rows,
            preferred_element_type=jnp.float32,
        )
        return ((new_highest, totals, accumulated), None)

    initial = (
        jnp.full((heads_here, tok_rows), -jnp.inf, jnp.float32),
        jnp.zeros((heads_here, tok_rows), jnp.float32),
        jnp.zeros((tok_rows, heads_here, VALUE_SIZE), jnp.float32),
    )
    carried = initial
    latent_piece = lax.all_gather(latent, "sp", axis=0, tiled=True)
    rope_piece = lax.all_gather(key_turned, "sp", axis=0, tiled=True)
    shard_count = latent_piece.shape[0] // tok_rows
    grouped = max(
        (
            factor
            for factor in range(1, shard_count + 1)
            if shard_count % factor == 0 and factor * tok_rows <= max(1024, tok_rows)
        )
    )
    block_rows = grouped * tok_rows
    blocks = (
        latent_piece.reshape(-1, block_rows, latent_piece.shape[1]),
        rope_piece.reshape(-1, block_rows, rope_piece.shape[1]),
    )
    carried, _ = lax.scan(absorb, carried, blocks)
    highest, totals, accumulated = carried
    attended = (
        (accumulated / totals.T[:, :, None])
        .reshape(tok_rows, heads_here * VALUE_SIZE)
        .astype(jnp.bfloat16)
    )
    projected = jnp.dot(attended, out_weight, preferred_element_type=jnp.float32).astype(
        jnp.bfloat16
    )
    summed = lax.psum(projected, "tp").astype(jnp.float32)
    mixed_all = residual.astype(jnp.float32) + summed
    normed_all = norm_rows(mixed_all, ffn_gain).astype(jnp.bfloat16)
    mixed_own = lax.dynamic_slice_in_dim(mixed_all, tp_index * own_rows, own_rows, 0)
    gate_piece = lax.all_gather(gate_weight, "sp", axis=0, tiled=True)
    up_piece = lax.all_gather(up_weight, "sp", axis=0, tiled=True)
    gate = jnp.dot(normed_all, gate_piece, preferred_element_type=jnp.float32)
    up_part = jnp.dot(normed_all, up_piece, preferred_element_type=jnp.float32)
    hidden = (jax.nn.silu(gate) * up_part).astype(jnp.bfloat16)
    terms = jnp.dot(
        hidden,
        lax.all_gather(down_weight, "sp", axis=1, tiled=True),
        preferred_element_type=jnp.float32,
    )
    ffn_own = lax.psum_scatter(
        terms.astype(jnp.bfloat16), "tp", scatter_dimension=0, tiled=True
    ).astype(jnp.float32)
    return (mixed_own + ffn_own).astype(jnp.bfloat16)


def solution(mesh):
    return jax.shard_map(
        local,
        mesh=mesh,
        in_specs=(
            P(("grp", "sp"), "tp"),
            P(("grp", "sp"), "tp"),
            P(("grp", "sp"), None),
            P(("grp", "sp"), None),
            P(),
            P(),
            P(),
            P(("grp", "sp"), None),
            P("tp", None),
            P(),
            P("sp", "tp"),
            P("sp", "tp"),
            P("tp", "sp"),
        ),
        out_specs=P(("grp", "sp", "tp"), None),
        check_vma=False,
    )
```
